32 devices in a mesh: sp: 8 (over z, y), dp: 4 (over x, core).
Axes of the slice: x: 2, y: 2, z: 4, core: 2. Of those that a mesh axis runs over, the one named last changes fastest.
Arguments:
- tokens: bfloat16 [4, 2560, 2048], P('dp', 'sp'), may hold values from -6 to 6
- w_query: bfloat16 [2048, 1024], P('dp', 'sp'), may hold values from -0.125 to 0.125
- w_key: bfloat16 [2048, 1024], P('dp', 'sp'), may hold values from -0.125 to 0.125
- w_value: bfloat16 [2048, 1024], P('dp', 'sp'), may hold values from -0.125 to 0.125
- w_output: bfloat16 [1024, 2048], P('sp', 'dp'), may hold values from -0.1875 to 0.1875
- qk_gain: float32 [2, 64], replicated, may hold values from 0.4 to 7
- decay_sums: float32 [4, 16, 2560], P('dp', 'sp'), may hold values from -512 to 0, as said below
Outputs:
- layer_out: bfloat16 [4, 2560, 2048], P('dp', 'sp')
The draws below stay inside these ranges and needn't reach their ends.
Inputs may be any that keep to these rules, and one draw needn't show every extreme that they name: `decay_sums`: each row is non-increasing along positions.
All inputs are finite; a program needn't handle non-finite values.
Results may differ from the reference program's by a relative error of at most 0.0075.
The reference program's roundings to bfloat16 on the way (of `query_proj`, `key_proj`, `value_proj`, `query_unit`, `key_unit`, `probs` and `head_out`) count: a program that leaves them out, or rounds other values in their place, can miss the bound.
Values may be sent and summed in bfloat16 or wider, within the bound.
A program may use at most 128 MiB of HBM per device.

```python
import jax
import jax.numpy as jnp
from jax import lax

D = 2048
HEADS = 16
HEAD_DIM = 64
TOK_DEV = 320
LENGTH = 2560
SEQS = 4


def draw_qk_gain(key, part):
    return jnp.clip(1.0 + 0.25 * jax.random.normal(key, (2, HEAD_DIM), jnp.float32), 0.4, 1.8)


def draw_decay_sums(key, part):
    streams = jax.random.split(key, 5)
    chance = 0.5
    quick = jax.random.bernoulli(streams[0], chance, (SEQS, HEADS, 1))
    quick_rate = 1.0 / jax.random.uniform(streams[1], (SEQS, HEADS, 1), jnp.float32, 30.0, 100.0)
    slow_rate = jax.random.uniform(streams[2], (SEQS, HEADS, 1), jnp.float32, 0.2, 0.8) / LENGTH
    rate = jnp.where(quick, quick_rate, slow_rate)
    spans = LENGTH // TOK_DEV
    factor = jnp.exp(jax.random.uniform(streams[3], (SEQS, HEADS, spans), jnp.float32, -1.05, 1.05))
    factor = jnp.repeat(factor, TOK_DEV, axis=2)
    rough = jax.random.uniform(streams[4], (SEQS, HEADS, LENGTH), jnp.float32, 0.2, 1.8)
    return -jnp.cumsum(rate * factor * rough, axis=2)


def steps_of(own_key, dims, shards, smallest, largest):
    level, own = 1.0, jax.random.fold_in(own_key, 6)
    for position, parts in shards:
        heights = jnp.exp(jax.random.uniform(jax.random.fold_in(own, position), (parts,), jnp.float32, smallest / len(shards), largest / len(shards)))
        level = level * jnp.repeat(heights, dims[position] // parts).reshape([-1 if axis == position else 1 for axis in range(len(dims))])
    return level


def normal_values(rng, extent, width, bound, pieces=(), held_as=jnp.bfloat16):
    level = steps_of(rng, extent, pieces, -0.22, 0.18) if pieces else 1.0
    drawn = jax.random.normal(rng, extent, jnp.float32) * width * level
    return jnp.minimum(jnp.maximum(drawn, -bound), bound).astype(held_as)


def setup_inputs(seed: int = 0) -> dict:
    key_of = jax.random.split(jax.random.key(seed), 8)
    return {
        "tokens": normal_values(key_of[0], (SEQS, LENGTH, D), 1.0, 6.0, ((0, 4), (1, 8))),
        "w_query": normal_values(key_of[1], (D, HEADS * HEAD_DIM), D ** -0.5, 0.125, ((0, 4), (1, 8))),
        "w_key": normal_values(key_of[2], (D, HEADS * HEAD_DIM), D ** -0.5, 0.125, ((0, 4), (1, 8))),
        "w_value": normal_values(key_of[3], (D, HEADS * HEAD_DIM), D ** -0.5, 0.125, ((0, 4), (1, 8))),
        "w_output": normal_values(key_of[4], (HEADS * HEAD_DIM, D), (HEADS * HEAD_DIM) ** -0.5, 0.1875, ((0, 8), (1, 4))),
        "qk_gain": draw_qk_gain(jax.random.fold_in(key_of[7], 71), 0),
        "decay_sums": draw_decay_sums(jax.random.fold_in(key_of[7], 71), 0),
    }


def normalize(values):
    values = values.astype(jnp.float32)
    return values * lax.rsqrt(lax.optimization_barrier(jnp.mean(values * values, axis=-1, keepdims=True)) + 1e-06)

def attend(query_unit, key_unit, value_rows, decay_rows):
    length = query_unit.shape[0]
    block = min(512, length)
    key_place = jnp.arange(length, dtype=jnp.int32)
    keys_wide = key_unit.astype(jnp.float32)
    values_wide = value_rows.astype(jnp.float32)

    def one_block(index):
        start = (index * block).astype(jnp.int32)
        query_block = lax.dynamic_slice_in_dim(query_unit, start, block, 0).astype(jnp.float32)
        decay_block = lax.dynamic_slice_in_dim(decay_rows, start, block, 1)
        scores = jnp.einsum('qhd,khd->hqk', query_block, keys_wide, precision=lax.Precision.HIGHEST)
        scores = scores + decay_block[:, :, None] - decay_rows[:, None, :]
        query_place = start + jnp.arange(block, dtype=jnp.int32)
        scores = jnp.where(key_place[None, None, :] <= query_place[None, :, None], scores, -jnp.inf)
        peak = lax.optimization_barrier(jnp.max(scores, axis=-1, keepdims=True))
        weights = jnp.exp(scores - peak)
        probs = (weights / lax.optimization_barrier(jnp.sum(weights, axis=-1, keepdims=True))).astype(jnp.bfloat16)
        return jnp.einsum('hqk,khd->qhd', probs.astype(jnp.float32), values_wide, precision=lax.Precision.HIGHEST)
    blocks = lax.map(one_block, jnp.arange(length // block, dtype=jnp.int32))
    return blocks.reshape(length, query_unit.shape[1], query_unit.shape[2])

def reference(tokens, w_query, w_key, w_value, w_output, qk_gain, decay_sums):

    def one_sequence(pair):
        own_rows, decay_rows = pair
        length = own_rows.shape[0]
        query_proj = jnp.dot(own_rows, w_query, preferred_element_type=jnp.float32).astype(jnp.bfloat16)
        key_proj = jnp.dot(own_rows, w_key, preferred_element_type=jnp.float32).astype(jnp.bfloat16)
        value_proj = jnp.dot(own_rows, w_value, preferred_element_type=jnp.float32).astype(jnp.bfloat16)
        query_proj = query_proj.reshape(length, HEADS, HEAD_DIM)
        key_proj = key_proj.reshape(length, HEADS, HEAD_DIM)
        value_proj = value_proj.reshape(length, HEADS, HEAD_DIM)
        query_unit = (normalize(query_proj) * qk_gain[0].astype(jnp.float32) * HEAD_DIM ** (-0.5)).astype(jnp.bfloat16)
        key_unit = (normalize(key_proj) * qk_gain[1].astype(jnp.float32)).astype(jnp.bfloat16)
        attended = attend(query_unit, key_unit, value_proj, decay_rows)
        head_out = normalize(attended).astype(jnp.bfloat16).reshape(length, HEADS * HEAD_DIM)
        return jnp.dot(head_out, w_output, preferred_element_type=jnp.float32).astype(jnp.bfloat16)
    return lax.map(one_sequence, (tokens, decay_sums))
```

```python
import functools

import jax
import jax.numpy as jnp
from jax import lax
from jax.experimental import pallas as pl
from jax.experimental.pallas import tpu as pltpu
from jax.sharding import PartitionSpec as P

EPS = 1e-06
DIMS_NT = (((1,), (1,)), ((), ()))
MESH = pl.DeviceIdType.MESH
CORES = 2


def layout(count, groups):
    tall = 4 if count % 4 == 0 else 1
    return tall, count // tall, groups // CORES


def layer_kernel(
    heads, width, count, groups,
    own_ref, wq_ref, wk_ref, wv_ref, slab_ref, gain_ref, decay_ref, out_ref,
    far_ref, unit_weight_ref, value_weight_ref, slabs_ref, unit_stage_ref, value_stage_ref,
    unit_ref, val_ref, key_ref, value_ref, done_ref, merged_ref,
    far_send, far_recv, wz_send, wx_send, wc_send, w_recv, move_send, move_recv,
    sz_send, sz_recv, sy_send, sy_recv, sx_send, sx_recv, sc_send, sc_recv, done_send, done_recv,
):
    rows, depth = own_ref.shape
    part = wq_ref.shape[0]
    owners = 2
    block = owners * rows
    wide = heads * width
    tall, broad, across = layout(count, groups)
    me, group = lax.axis_index("sp"), lax.axis_index("dp")
    z, y = me // broad, lax.rem(me, broad)
    x, core = group // CORES, lax.rem(group, CORES)
    partner = x * CORES + 1 - core

    def plane(shift):
        return lax.rem(z + shift, tall)

    def along_x(shift):
        return lax.rem(x + shift, across)

    def along_y(shift):
        return lax.rem(y + shift, broad)

    barrier = pltpu.get_barrier_semaphore()
    for shift in range(1, count):
        other = lax.rem(me + shift, count)
        pl.semaphore_signal(barrier, inc=1, device_id={"sp": other}, device_id_type=MESH)
    for shift in range(1, groups):
        peer = lax.rem(group + shift, groups)
        pl.semaphore_signal(barrier, inc=1, device_id={"dp": peer}, device_id_type=MESH)
    pl.semaphore_wait(barrier, count + groups - 2)

    def remote(source, target, out_sem, in_sem, device):
        return pltpu.make_async_remote_copy(
            src_ref=source, dst_ref=target, send_sem=out_sem, recv_sem=in_sem,
            device_id=device, device_id_type=MESH,
        )

    tokens = [
        remote(
            own_ref, far_ref.at[broad - shift - 1], far_send.at[shift - 1],
            far_recv.at[broad - shift - 1], {"sp": z * broad + along_y(shift)},
        )
        for shift in range(1, broad)
    ]

    chunks = [("unit", 0), ("value", 0)] + [("unit", head) for head in range(1, heads)]
    weights = [
        unit_weight_ref.at[head] if kind == "unit" else value_weight_ref for kind, head in chunks
    ]

    def weight(number, level, owner, out_sem, device):
        piece = weights[number].at[level, owner]
        return remote(piece, piece, out_sem, w_recv.at[number, level, owner], device)

    def up(number, level):
        return weight(
            number, level, group, wz_send.at[number, level, 0], {"sp": (z + 1) * broad + y}
        )

    def down(number, level):
        return weight(
            number, level, group, wz_send.at[number, level, 1], {"sp": (z - 1) * broad + y}
        )

    def sideways(number, level):
        return [
            weight(
                number, level, group, wx_send.at[number, level, shift - 1],
                {"dp": along_x(shift) * CORES + core},
            )
            for shift in range(1, across)
        ]

    def to_core(number, level, column):
        return weight(
            number, level, column * CORES + core, wc_send.at[number, level, column],
            {"dp": partner},
        )

    def own_weight(number):
        @pl.when(z + 1 < tall)
        def _():
            up(number, z).start()

        @pl.when(z > 0)
        def _():
            down(number, z).start()

        for copy in sideways(number, z):
            copy.start()
        to_core(number, z, x).start()

    def relay(number, distance):
        @pl.when(z - distance >= 0)
        def _():
            level = z - distance
            up(number, level).wait_recv()

            @pl.when(z + 1 < tall)
            def _():
                up(number, level).start()

            for copy in sideways(number, level):
                copy.start()
            to_core(number, level, x).start()

        @pl.when(z + distance < tall)
        def _():
            level = z + distance
            down(number, level).wait_recv()

            @pl.when(z > 0)
            def _():
                down(number, level).start()

            for copy in sideways(number, level):
                copy.start()
            to_core(number, level, x).start()

    def relay_core(number):
        for turn in range(tall):
            for shift in range(1, across):
                level, column = plane(turn), along_x(shift)
                copy = to_core(number, level, column)
                weight(
                    number, level, column * CORES + core, wc_send.at[number, level, column],
                    {"dp": partner},
                ).wait_recv()
                copy.start()

    def gathered(number):
        for turn in range(tall):
            for column in range(across):
                level = plane(turn)
                weight(
                    number, level, column * CORES + 1 - core, wc_send.at[number, level, column],
                    {"dp": partner},
                ).wait_recv()

    def weights_sent(number):
        for turn in range(tall):
            level = plane(turn)

            @pl.when((level <= z) & (z + 1 < tall))
            def _():
                up(number, level).wait_send()

            @pl.when((level >= z) & (z > 0))
            def _():
                down(number, level).wait_send()

            for copy in sideways(number, level):
                copy.wait_send()
            for column in range(across):
                to_core(number, level, column).wait_send()

    lane = lax.broadcasted_iota(jnp.int32, (rows, 2 * width), 1)
    gain = jnp.concatenate([gain_ref[0:1, :] * width ** (-0.5), gain_ref[1:2, :]], axis=1)

    def unit(values):
        values = values.astype(jnp.bfloat16).astype(jnp.float32)
        squares = values * values
        first = jnp.sum(jnp.where(lane < width, squares, 0.0), axis=-1, keepdims=True)
        second = jnp.sum(jnp.where(lane < width, 0.0, squares), axis=-1, keepdims=True)
        scale = jnp.where(
            lane < width, lax.rsqrt(first / width + EPS), lax.rsqrt(second / width + EPS)
        )
        return values * scale * gain

    def move(number, turn, side):
        kind, head = chunks[number]
        source = z * broad + along_y(side)
        place = pl.ds(pl.multiple_of(source * rows, rows), rows)
        if kind == "unit":
            staged, target = unit_stage_ref.at[head, side, turn], unit_ref.at[head, place]
        else:
            staged, target = value_stage_ref.at[side, turn], val_ref.at[place]
        return remote(
            staged, target, move_send.at[number, side, turn], move_recv.at[number, source],
            {"sp": plane(turn) * broad + y},
        )

    turns = sorted(range(tall), key=lambda turn: (turn == 0, turn != tall // 2))

    def project(number, side):
        kind, head = chunks[number]
        values = own_ref[...] if side == 0 else far_ref[side - 1]
        lanes = weights[number].shape[-1]
        bunch = 2 if lanes % 128 == 0 and tall % 2 == 0 else 1
        for first in range(0, tall, bunch):
            some = turns[first : first + bunch]
            columns = [
                weights[number][plane(turn)].reshape(depth, lanes) for turn in some
            ]
            result = jnp.dot(
                values, columns[0] if bunch == 1 else jnp.concatenate(columns, axis=1),
                preferred_element_type=jnp.float32,
            )
            for index, turn in enumerate(some):
                piece = result[:, index * lanes : (index + 1) * lanes]
                piece = (unit(piece) if kind == "unit" else piece).astype(jnp.bfloat16)
                if turn:
                    if kind == "unit":
                        unit_stage_ref[head, side, turn] = piece
                    else:
                        value_stage_ref[side, turn] = piece
                    move(number, turn, side).start()
                else:
                    place = (z * broad + along_y(side)) * rows
                    place = pl.ds(pl.multiple_of(place, rows), rows)
                    if kind == "unit":
                        unit_ref[head, place, :] = piece
                    else:
                        val_ref[place, :] = piece

    def moved(number):
        kind, head = chunks[number]
        for turn in range(1, tall):
            for column in range(broad):
                source = plane(turn) * broad + column
                place = pl.ds(pl.multiple_of(source * rows, rows), rows)
                target = unit_ref.at[head, place] if kind == "unit" else val_ref.at[place]
                remote(
                    target, target, move_send.at[number, 0, turn], move_recv.at[number, source],
                    {"sp": source},
                ).wait_recv()

    tall_slab = slab_ref.shape[0]

    def slab_z(level, way):
        place = pl.ds(pl.multiple_of(level * tall_slab, tall_slab), tall_slab)
        piece = slabs_ref.at[group, y, place]
        return remote(
            piece, piece, sz_send.at[level, way], sz_recv.at[level],
            {"sp": (z + 1 - 2 * way) * broad + y},
        )

    def slab_relay(distance):
        for way in range(2):
            level = z - distance if way == 0 else z + distance
            inside = (level >= 0) if way == 0 else (level < tall)
            onward = (z + 1 < tall) if way == 0 else (z > 0)
            if distance:
                @pl.when(inside)
                def _():
                    slab_z(level, way).wait_recv()

            @pl.when(inside & onward)
            def _():
                slab_z(level, way).start()

    def slab_y(shift):
        piece = slabs_ref.at[group, y]
        return remote(
            piece, piece, sy_send.at[shift - 1], sy_recv.at[y],
            {"sp": z * broad + along_y(shift)},
        )

    def slab_x(column, shift):
        piece = slabs_ref.at[group, column]
        return remote(
            piece, piece, sx_send.at[column, shift - 1], sx_recv.at[x, column],
            {"dp": along_x(shift) * CORES + core},
        )

    def slab_core(level, column):
        piece = slabs_ref.at[level * CORES + core, column]
        return remote(
            piece, piece, sc_send.at[level, column], sc_recv.at[level, column], {"dp": partner}
        )

    def slab_spread(column):
        for shift in range(1, across):
            slab_x(column, shift).start()
        slab_core(x, column).start()

    def slabs_of_y():
        for shift in range(1, broad):
            slab_y(shift).start()
        slab_spread(y)

    def slabs_from_y():
        for shift in range(1, broad):
            column = along_y(shift)
            piece = slabs_ref.at[group, column]
            remote(
                piece, piece, sy_send.at[shift - 1], sy_recv.at[column], {"sp": me}
            ).wait_recv()
            slab_spread(column)

    def slabs_from_x():
        for turn in range(broad):
            column = along_y(turn)
            for shift in range(1, across):
                level = along_x(shift)
                piece = slabs_ref.at[level * CORES + core, column]
                remote(
                    piece, piece, sx_send.at[column, shift - 1], sx_recv.at[level, column],
                    {"dp": group},
                ).wait_recv()
                slab_core(level, column).start()

    def slabs_from_core():
        for level in range(across):
            for column in range(broad):
                piece = slabs_ref.at[level * CORES + 1 - core, column]
                remote(
                    piece, piece, sc_send.at[level, column], sc_recv.at[level, column],
                    {"dp": partner},
                ).wait_recv()

    for number, (kind, head) in enumerate(chunks):
        if kind == "unit":
            low = head * width
            pair = [ref[:, low : low + width].astype(jnp.float32) for ref in (wq_ref, wk_ref)]
            unit_weight_ref[head, z, group] = jnp.concatenate(pair, axis=1).astype(jnp.bfloat16)
        else:
            value_weight_ref[z, group] = wv_ref[...]
        own_weight(number)
        if number == 0:
            for copy in tokens:
                copy.start()
    slabs_ref[group, y, pl.ds(pl.multiple_of(z * tall_slab, tall_slab), tall_slab), :] = slab_ref[
        ...
    ]

    def relays(number):
        for distance in range(1, tall):
            relay(number, distance)

    def ready(number):
        relay_core(number)
        gathered(number)

    last = len(chunks) - 1
    relays(0)
    ready(0)
    for number in range(1, len(chunks)):
        relays(number)
        project(number - 1, 0)
        ready(number)
    for number in range(last):
        if number == 0:
            for copy in tokens:
                copy.wait_recv()
        for side in range(1, broad):
            project(number, side)
    slab_relay(0)
    for side in range(broad):
        project(last, side)
    for distance in range(1, tall):
        slab_relay(distance)
    slabs_of_y()
    for number in range(len(chunks)):
        moved(number)

    def remote_done(source, owner):
        return remote(
            done_ref.at[owner], merged_ref.at[source], done_send.at[owner], done_recv.at[source],
            {"sp": owner},
        )

    def one_block(index, unused):
        place = pl.ds(pl.multiple_of(index * block, block), block)
        values_turned = val_ref[place, :].astype(jnp.float32).T
        lane = lax.broadcasted_iota(jnp.int32, (block, 2 * width), 1)
        ones_lanes = jnp.where(lane < 3, 1.0, 0.0)
        sub = lax.broadcasted_iota(jnp.int32, (2 * width, block), 0)
        ones_rows = jnp.where(
            lax.broadcasted_iota(jnp.int32, (16, block), 0) == 0, 1.0, 0.0
        )
        queries = []
        for head in range(heads):
            low = head * width
            units = unit_ref[head, place, :].astype(jnp.float32)
            decay = -decay_ref[head : head + 1, place]
            first = decay.astype(jnp.bfloat16).astype(jnp.float32)
            rest = decay - first
            second = rest.astype(jnp.bfloat16).astype(jnp.float32)
            third = rest - second
            parts = jnp.where(
                sub == 0, first, jnp.where(sub == 1, second, jnp.where(sub == 2, third, 0.0))
            ).T
            turned_units = pltpu.roll(units, width, 1)
            queries.append(jnp.where(lane < width, ones_lanes, turned_units).astype(jnp.bfloat16))
            key_ref[head, place, :] = jnp.where(lane < width, parts, units).astype(jnp.bfloat16)
            value_ref[head, index] = jnp.concatenate(
                [values_turned[low : low + width], ones_rows], axis=0
            ).astype(jnp.bfloat16)

        def step(column, carry, masked):
            fresh = []
            for head in range(heads):
                peak, total = carry[head]
                keys = key_ref[head, pl.ds(pl.multiple_of(column * block, block), block), :]
                scores = lax.dot_general(
                    keys, queries[head], DIMS_NT, preferred_element_type=jnp.float32
                )
                if masked:
                    key_place = lax.broadcasted_iota(jnp.int32, scores.shape, 0)
                    query_place = lax.broadcasted_iota(jnp.int32, scores.shape, 1)
                    scores = jnp.where(key_place <= query_place, scores, -jnp.inf)
                higher = jnp.maximum(peak, jnp.max(scores, axis=0, keepdims=True))
                probs = jnp.exp(scores - higher).astype(jnp.bfloat16)
                total = total * jnp.exp(peak - higher) + jnp.dot(
                    value_ref[head, column], probs, preferred_element_type=jnp.float32
                )
                fresh.append((higher, total))
            return tuple(fresh)

        start = tuple(
            (
                jnp.full((1, block), -1e30, jnp.float32),
                jnp.zeros((width + 16, block), jnp.float32),
            )
            for _ in range(heads)
        )
        carry = step(index, start, True)
        carry = lax.fori_loop(0, index, lambda column, c: step(column, c, False), carry)
        outs = []
        for head in range(heads):
            total = carry[head][1]
            mixed, norm = total[:width], total[width : width + 1]
            scale = lax.rsqrt(jnp.mean(mixed * mixed, axis=0, keepdims=True) + EPS * norm * norm)
            outs.append(mixed * scale)
        turned = jnp.concatenate(outs, axis=0).T.astype(jnp.bfloat16)
        for part_index in range(owners):
            owner = index * owners + part_index
            done_ref[owner] = turned[part_index * rows : (part_index + 1) * rows]

            @pl.when(owner != me)
            def _():
                remote_done(me, owner).start()

        @pl.when(index == 1)
        def _():
            slabs_from_y()

        @pl.when(index == 2)
        def _():
            slabs_from_x()

        return unused

    lax.fori_loop(0, count // owners, one_block, 0)
    merged_ref[me] = done_ref[me]
    slabs_from_core()
    for shift in range(1, count):
        other = lax.rem(me + shift, count)
        remote_done(other, other).wait_recv()
    merged = jnp.concatenate(
        [merged_ref[level * broad + column] for column in range(broad) for level in range(tall)],
        axis=1,
    )
    columns = slab_ref.shape[1]
    for place in range(groups):
        out_ref[:, place * columns : (place + 1) * columns] = jnp.dot(
            merged, slabs_ref[place].reshape(-1, columns), preferred_element_type=jnp.float32
        ).astype(out_ref.dtype)

    for copy in tokens:
        copy.wait_send()
    for number in range(len(chunks)):
        weights_sent(number)
        for side in range(broad):
            for turn in range(1, tall):
                move(number, turn, side).wait_send()
    for distance in range(tall):
        for way in range(2):
            level = z - distance if way == 0 else z + distance
            inside = (level >= 0) if way == 0 else (level < tall)
            onward = (z + 1 < tall) if way == 0 else (z > 0)

            @pl.when(inside & onward)
            def _():
                slab_z(level, way).wait_send()

    for shift in range(1, broad):
        slab_y(shift).wait_send()
    for column in range(broad):
        for shift in range(1, across):
            slab_x(column, shift).wait_send()
        for level in range(across):
            slab_core(level, column).wait_send()
    for shift in range(1, count):
        remote_done(me, lax.rem(me + shift, count)).wait_send()


def on_device(tokens, w_query, w_key, w_value, w_output, qk_gain, decay_sums):
    own_rows, decay_rows = tokens[0], decay_sums[0]
    count, groups = lax.axis_size("sp"), lax.axis_size("dp")
    tall, broad, across = layout(count, groups)
    rows, depth = own_rows.shape
    part = w_query.shape[0]
    heads, width = decay_rows.shape[0], qk_gain.shape[1]
    wide, length, block = heads * width, count * rows, 2 * rows
    tall_slab, columns = w_output.shape
    bf16, sem, chunks = jnp.bfloat16, pltpu.SemaphoreType.DMA, heads + 1
    others, beside = max(broad - 1, 1), max(across - 1, 1)
    result = pl.pallas_call(
        functools.partial(layer_kernel, heads, width, count, groups),
        out_shape=jax.ShapeDtypeStruct((rows, depth), bf16),
        in_specs=[pl.BlockSpec(memory_space=pltpu.VMEM)] * 7,
        out_specs=pl.BlockSpec(memory_space=pltpu.VMEM),
        scratch_shapes=[
            pltpu.VMEM((others, rows, depth), bf16),
            pltpu.VMEM((heads, tall, groups, part, 2 * width), bf16),
            pltpu.VMEM((tall, groups, part, wide), bf16),
            pltpu.VMEM((groups, broad, tall * tall_slab, columns), bf16),
            pltpu.VMEM((heads, broad, tall, rows, 2 * width), bf16),
            pltpu.VMEM((broad, tall, rows, wide), bf16),
            pltpu.VMEM((heads, length, 2 * width), bf16),
            pltpu.VMEM((length, wide), bf16),
            pltpu.VMEM((heads, length, 2 * width), bf16),
            pltpu.VMEM((heads, length // block, width + 16, block), bf16),
            pltpu.VMEM((count, rows, wide), bf16),
            pltpu.VMEM((count, rows, wide), bf16),
            sem((others,)), sem((others,)),
            sem((chunks, tall, 2)), sem((chunks, tall, beside)), sem((chunks, tall, across)),
            sem((chunks, tall, groups)),
            sem((chunks, broad, tall)), sem((chunks, count)),
            sem((tall, 2)), sem((tall,)), sem((others,)), sem((broad,)),
            sem((broad, beside)), sem((across, broad)), sem((across, broad)), sem((across, broad)),
            sem((count,)), sem((count,)),
        ],
        compiler_params=pltpu.CompilerParams(
            collective_id=0, has_side_effects=True, vmem_limit_bytes=60 * 1024 * 1024
        ),
    )(own_rows, w_query, w_key, w_value, w_output, qk_gain, decay_rows)
    return result[None]


def solution(mesh):
    placed = (
        P("dp", "sp", None),
        P("dp", "sp"),
        P("dp", "sp"),
        P("dp", "sp"),
        P("sp", "dp"),
        P(),
        P("dp", "sp", None),
    )
    return jax.shard_map(
        on_device, mesh=mesh, in_specs=placed, out_specs=P("dp", "sp", None), check_vma=False
    )
```

```python
import functools

import jax
import jax.numpy as jnp
from jax import lax
from jax.experimental import pallas as pl
from jax.experimental.pallas import tpu as pltpu
from jax.sharding import PartitionSpec as P

EPS = 1e-06
DIMS_NT = (((1,), (1,)), ((), ()))
MESH = pl.DeviceIdType.MESH
CORES = 2


def layout(count, groups):
    tall = 4 if count % 4 == 0 else 1
    return tall, count // tall, groups // CORES


def layer_kernel(
    heads, width, count, groups,
    own_ref, wq_ref, wk_ref, wv_ref, slab_ref, gain_ref, decay_ref, out_ref,
    far_ref, unit_weight_ref, value_weight_ref, slabs_ref, unit_stage_ref, value_stage_ref,
    unit_ref, val_ref, key_ref, value_ref, done_ref, merged_ref,
    far_send, far_recv, wz_send, wx_send, wc_send, w_recv, move_send, move_recv,
    sz_send, sz_recv, sy_send, sy_recv, sx_send, sx_recv, sc_send, sc_recv, done_send, done_recv,
):
    rows, depth = own_ref.shape
    part = wq_ref.shape[0]
    owners = 2
    block = owners * rows
    wide = heads * width
    tall, broad, across = layout(count, groups)
    me, group = lax.axis_index("sp"), lax.axis_index("dp")
    z, y = me // broad, lax.rem(me, broad)
    x, core = group // CORES, lax.rem(group, CORES)
    partner = x * CORES + 1 - core

    def plane(shift):
        return lax.rem(z + shift, tall)

    def along_x(shift):
        return lax.rem(x + shift, across)

    def along_y(shift):
        return lax.rem(y + shift, broad)

    barrier = pltpu.get_barrier_semaphore()
    for shift in range(1, count):
        other = lax.rem(me + shift, count)
        pl.semaphore_signal(barrier, inc=1, device_id={"sp": other}, device_id_type=MESH)
    for shift in range(1, groups):
        peer = lax.rem(group + shift, groups)
        pl.semaphore_signal(barrier, inc=1, device_id={"dp": peer}, device_id_type=MESH)
    pl.semaphore_wait(barrier, count + groups - 2)

    def remote(source, target, out_sem, in_sem, device):
        return pltpu.make_async_remote_copy(
            src_ref=source, dst_ref=target, send_sem=out_sem, recv_sem=in_sem,
            device_id=device, device_id_type=MESH,
        )

    tokens = [
        remote(
            own_ref, far_ref.at[broad - shift - 1], far_send.at[shift - 1],
            far_recv.at[broad - shift - 1], {"sp": z * broad + along_y(shift)},
        )
        for shift in range(1, broad)
    ]

    chunks = [("unit", 0), ("value", 0)] + [("unit", head) for head in range(1, heads)]
    weights = [
        unit_weight_ref.at[head] if kind == "unit" else value_weight_ref for kind, head in chunks
    ]

    def weight(number, level, owner, out_sem, device):
        piece = weights[number].at[level, owner]
        return remote(piece, piece, out_sem, w_recv.at[number, level, owner], device)

    def up(number, level):
        return weight(
            number, level, group, wz_send.at[number, level, 0], {"sp": (z + 1) * broad + y}
        )

    def down(number, level):
        return weight(
            number, level, group, wz_send.at[number, level, 1], {"sp": (z - 1) * broad + y}
        )

    def sideways(number, level):
        return [
            weight(
                number, level, group, wx_send.at[number, level, shift - 1],
                {"dp": along_x(shift) * CORES + core},
            )
            for shift in range(1, across)
        ]

    def to_core(number, level, column):
        return weight(
            number, level, column * CORES + core, wc_send.at[number, level, column],
            {"dp": partner},
        )

    def own_along_z(number):
        @pl.when(z + 1 < tall)
        def _():
            up(number, z).start()

        @pl.when(z > 0)
        def _():
            down(number, z).start()

    def spread(number, level):
        for copy in sideways(number, level):
            copy.start()
        to_core(number, level, x).start()

    def relay(number, distance, onward=True, across_too=True):
        for way, step in enumerate((up, down)):
            level = z - distance if way == 0 else z + distance
            inside = (level >= 0) if way == 0 else (level < tall)
            more = (z + 1 < tall) if way == 0 else (z > 0)

            @pl.when(inside)
            def _():
                if onward:
                    step(number, level).wait_recv()

                    @pl.when(more)
                    def _():
                        step(number, level).start()

                if across_too:
                    spread(number, level)

    def relay_core(number):
        for turn in range(tall):
            for shift in range(1, across):
                level, column = plane(turn), along_x(shift)
                copy = to_core(number, level, column)
                weight(
                    number, level, column * CORES + core, wc_send.at[number, level, column],
                    {"dp": partner},
                ).wait_recv()
                copy.start()

    def gathered(number):
        for turn in range(tall):
            for column in range(across):
                level = plane(turn)
                weight(
                    number, level, column * CORES + 1 - core, wc_send.at[number, level, column],
                    {"dp": partner},
                ).wait_recv()

    def weights_sent(number):
        for turn in range(tall):
            level = plane(turn)

            @pl.when((level <= z) & (z + 1 < tall))
            def _():
                up(number, level).wait_send()

            @pl.when((level >= z) & (z > 0))
            def _():
                down(number, level).wait_send()

            for copy in sideways(number, level):
                copy.wait_send()
            for column in range(across):
                to_core(number, level, column).wait_send()

    lane = lax.broadcasted_iota(jnp.int32, (rows, 2 * width), 1)
    gain = jnp.concatenate([gain_ref[0:1, :] * width ** (-0.5), gain_ref[1:2, :]], axis=1)

    def unit(values):
        values = values.astype(jnp.bfloat16).astype(jnp.float32)
        squares = values * values
        first = jnp.sum(jnp.where(lane < width, squares, 0.0), axis=-1, keepdims=True)
        second = jnp.sum(jnp.where(lane < width, 0.0, squares), axis=-1, keepdims=True)
        scale = jnp.where(
            lane < width, lax.rsqrt(first / width + EPS), lax.rsqrt(second / width + EPS)
        )
        return values * scale * gain

    def move(number, turn, side):
        kind, head = chunks[number]
        source = z * broad + along_y(side)
        place = pl.ds(pl.multiple_of(source * rows, rows), rows)
        if kind == "unit":
            staged, target = unit_stage_ref.at[head, side, turn], unit_ref.at[head, place]
        else:
            staged, target = value_stage_ref.at[side, turn], val_ref.at[place]
        return remote(
            staged, target, move_send.at[number, side, turn], move_recv.at[number, source],
            {"sp": plane(turn) * broad + y},
        )

    turns = sorted(range(tall), key=lambda turn: (turn == 0, turn != tall // 2))

    def project(number, side):
        kind, head = chunks[number]
        values = own_ref[...] if side == 0 else far_ref[side - 1]
        lanes = weights[number].shape[-1]
        bunch = 2 if lanes % 128 == 0 and tall % 2 == 0 else 1
        for first in range(0, tall, bunch):
            some = turns[first : first + bunch]
            columns = [
                weights[number][plane(turn)].reshape(depth, lanes) for turn in some
            ]
            result = jnp.dot(
                values, columns[0] if bunch == 1 else jnp.concatenate(columns, axis=1),
                preferred_element_type=jnp.float32,
            )
            for index, turn in enumerate(some):
                piece = result[:, index * lanes : (index + 1) * lanes]
                piece = (unit(piece) if kind == "unit" else piece).astype(jnp.bfloat16)
                if turn:
                    if kind == "unit":
                        unit_stage_ref[head, side, turn] = piece
                    else:
                        value_stage_ref[side, turn] = piece
                    move(number, turn, side).start()
                else:
                    place = (z * broad + along_y(side)) * rows
                    place = pl.ds(pl.multiple_of(place, rows), rows)
                    if kind == "unit":
                        unit_ref[head, place, :] = piece
                    else:
                        val_ref[place, :] = piece

    def moved(number):
        kind, head = chunks[number]
        for turn in range(1, tall):
            for column in range(broad):
                source = plane(turn) * broad + column
                place = pl.ds(pl.multiple_of(source * rows, rows), rows)
                target = unit_ref.at[head, place] if kind == "unit" else val_ref.at[place]
                remote(
                    target, target, move_send.at[number, 0, turn], move_recv.at[number, source],
                    {"sp": source},
                ).wait_recv()

    tall_slab = slab_ref.shape[0]

    def slab_z(level, way):
        place = pl.ds(pl.multiple_of(level * tall_slab, tall_slab), tall_slab)
        piece = slabs_ref.at[group, y, place]
        return remote(
            piece, piece, sz_send.at[level, way], sz_recv.at[level],
            {"sp": (z + 1 - 2 * way) * broad + y},
        )

    def slab_relay(distance):
        for way in range(2):
            level = z - distance if way == 0 else z + distance
            inside = (level >= 0) if way == 0 else (level < tall)
            onward = (z + 1 < tall) if way == 0 else (z > 0)
            if distance:
                @pl.when(inside)
                def _():
                    slab_z(level, way).wait_recv()

            @pl.when(inside & onward)
            def _():
                slab_z(level, way).start()

    def slab_x(shift):
        piece = slabs_ref.at[group, y]
        return remote(
            piece, piece, sx_send.at[shift - 1], sx_recv.at[x],
            {"dp": along_x(shift) * CORES + core},
        )

    def slab_y(level, shift):
        piece = slabs_ref.at[level * CORES + core, y]
        return remote(
            piece, piece, sy_send.at[level, shift - 1], sy_recv.at[level, y],
            {"sp": z * broad + along_y(shift)},
        )

    def slab_core(level, column):
        piece = slabs_ref.at[level * CORES + core, column]
        return remote(
            piece, piece, sc_send.at[level, column], sc_recv.at[level, column], {"dp": partner}
        )

    def slab_spread(level):
        for shift in range(1, broad):
            slab_y(level, shift).start()
        slab_core(level, y).start()

    def slabs_of_y():
        for shift in range(1, across):
            slab_x(shift).start()
        slab_spread(x)

    def slabs_from_x():
        for shift in range(1, across):
            level = along_x(shift)
            piece = slabs_ref.at[level * CORES + core, y]
            remote(
                piece, piece, sx_send.at[shift - 1], sx_recv.at[level], {"dp": group}
            ).wait_recv()
            slab_spread(level)

    def slabs_from_y():
        for turn in range(across):
            level = along_x(turn)
            for shift in range(1, broad):
                column = along_y(shift)
                piece = slabs_ref.at[level * CORES + core, column]
                remote(
                    piece, piece, sy_send.at[level, shift - 1], sy_recv.at[level, column],
                    {"sp": me},
                ).wait_recv()
                slab_core(level, column).start()

    def slabs_from_core():
        for level in range(across):
            for column in range(broad):
                piece = slabs_ref.at[level * CORES + 1 - core, column]
                remote(
                    piece, piece, sc_send.at[level, column], sc_recv.at[level, column],
                    {"dp": partner},
                ).wait_recv()

    for number, (kind, head) in enumerate(chunks):
        if kind == "unit":
            low = head * width
            pair = [ref[:, low : low + width].astype(jnp.float32) for ref in (wq_ref, wk_ref)]
            unit_weight_ref[head, z, group] = jnp.concatenate(pair, axis=1).astype(jnp.bfloat16)
        else:
            value_weight_ref[z, group] = wv_ref[...]
        if number < 2:
            own_along_z(number)
            spread(number, z)
        if number == 0:
            for copy in tokens:
                copy.start()
    slabs_ref[group, y, pl.ds(pl.multiple_of(z * tall_slab, tall_slab), tall_slab), :] = slab_ref[
        ...
    ]

    def ready(number):
        relay_core(number)
        gathered(number)

    last = len(chunks) - 1
    rest = range(2, len(chunks))
    for distance in range(1, tall):
        relay(0, distance)
        if distance == 1:
            relay(1, 1, across_too=False)
            for number in rest:
                own_along_z(number)
        elif distance == 2:
            relay(1, 1, onward=False)
            relay(1, 2, across_too=False)
    for number in rest:
        relay(number, 1, across_too=False)
    if tall > 2:
        relay(1, 2, onward=False)
    ready(0)
    for distance in range(3, tall):
        relay(1, distance)
    project(0, 0)
    for number in rest:
        spread(number, z)
        relay(number, 1, onward=False)
        if tall > 2:
            relay(number, 2)
    ready(1)
    for number in rest:
        for distance in range(3, tall):
            relay(number, distance)
    project(1, 0)
    slab_relay(0)
    for copy in tokens:
        copy.wait_recv()
    for number in range(2):
        for side in range(1, broad):
            project(number, side)
    for distance in range(1, tall):
        slab_relay(distance)
    slabs_of_y()
    for number in rest:
        ready(number)
        for side in range(broad):
            project(number, side)
    for number in range(len(chunks)):
        moved(number)

    def remote_done(source, owner):
        return remote(
            done_ref.at[owner], merged_ref.at[source], done_send.at[owner], done_recv.at[source],
            {"sp": owner},
        )

    def one_block(index, unused):
        place = pl.ds(pl.multiple_of(index * block, block), block)
        values_turned = val_ref[place, :].astype(jnp.float32).T
        lane = lax.broadcasted_iota(jnp.int32, (block, 2 * width), 1)
        ones_lanes = jnp.where(lane < 3, 1.0, 0.0)
        sub = lax.broadcasted_iota(jnp.int32, (2 * width, block), 0)
        ones_rows = jnp.where(
            lax.broadcasted_iota(jnp.int32, (16, block), 0) == 0, 1.0, 0.0
        )
        queries = []
        for head in range(heads):
            low = head * width
            units = unit_ref[head, place, :].astype(jnp.float32)
            decay = -decay_ref[head : head + 1, place]
            first = decay.astype(jnp.bfloat16).astype(jnp.float32)
            rest = decay - first
            second = rest.astype(jnp.bfloat16).astype(jnp.float32)
            third = rest - second
            parts = jnp.where(
                sub == 0, first, jnp.where(sub == 1, second, jnp.where(sub == 2, third, 0.0))
            ).T
            turned_units = pltpu.roll(units, width, 1)
            queries.append(jnp.where(lane < width, ones_lanes, turned_units).astype(jnp.bfloat16))
            key_ref[head, place, :] = jnp.where(lane < width, parts, units).astype(jnp.bfloat16)
            value_ref[head, index] = jnp.concatenate(
                [values_turned[low : low + width], ones_rows], axis=0
            ).astype(jnp.bfloat16)

        def step(column, carry, masked):
            fresh = []
            for head in range(heads):
                peak, total = carry[head]
                keys = key_ref[head, pl.ds(pl.multiple_of(column * block, block), block), :]
                scores = lax.dot_general(
                    keys, queries[head], DIMS_NT, preferred_element_type=jnp.float32
                )
                if masked:
                    key_place = lax.broadcasted_iota(jnp.int32, scores.shape, 0)
                    query_place = lax.broadcasted_iota(jnp.int32, scores.shape, 1)
                    scores = jnp.where(key_place <= query_place, scores, -jnp.inf)
                higher = jnp.maximum(peak, jnp.max(scores, axis=0, keepdims=True))
                probs = jnp.exp(scores - higher).astype(jnp.bfloat16)
                total = total * jnp.exp(peak - higher) + jnp.dot(
                    value_ref[head, column], probs, preferred_element_type=jnp.float32
                )
                fresh.append((higher, total))
            return tuple(fresh)

        start = tuple(
            (
                jnp.full((1, block), -1e30, jnp.float32),
                jnp.zeros((width + 16, block), jnp.float32),
            )
            for _ in range(heads)
        )
        carry = step(index, start, True)
        carry = lax.fori_loop(0, index, lambda column, c: step(column, c, False), carry)
        outs = []
        for head in range(heads):
            total = carry[head][1]
            mixed, norm = total[:width], total[width : width + 1]
            scale = lax.rsqrt(jnp.mean(mixed * mixed, axis=0, keepdims=True) + EPS * norm * norm)
            outs.append(mixed * scale)
        turned = jnp.concatenate(outs, axis=0).T.astype(jnp.bfloat16)
        for part_index in range(owners):
            owner = index * owners + part_index
            done_ref[owner] = turned[part_index * rows : (part_index + 1) * rows]

            @pl.when(owner != me)
            def _():
                remote_done(me, owner).start()

        @pl.when(index == 1)
        def _():
            slabs_from_x()

        @pl.when(index == 3)
        def _():
            slabs_from_y()

        return unused

    lax.fori_loop(0, count // owners, one_block, 0)
    merged_ref[me] = done_ref[me]
    slabs_from_core()
    for shift in range(1, count):
        other = lax.rem(me + shift, count)
        remote_done(other, other).wait_recv()
    merged = jnp.concatenate(
        [merged_ref[level * broad + column] for column in range(broad) for level in range(tall)],
        axis=1,
    )
    columns = slab_ref.shape[1]
    for place in range(groups):
        out_ref[:, place * columns : (place + 1) * columns] = jnp.dot(
            merged, slabs_ref[place].reshape(-1, columns), preferred_element_type=jnp.float32
        ).astype(out_ref.dtype)

    for copy in tokens:
        copy.wait_send()
    for number in range(len(chunks)):
        weights_sent(number)
        for side in range(broad):
            for turn in range(1, tall):
                move(number, turn, side).wait_send()
    for distance in range(tall):
        for way in range(2):
            level = z - distance if way == 0 else z + distance
            inside = (level >= 0) if way == 0 else (level < tall)
            onward = (z + 1 < tall) if way == 0 else (z > 0)

            @pl.when(inside & onward)
            def _():
                slab_z(level, way).wait_send()

    for shift in range(1, across):
        slab_x(shift).wait_send()
    for level in range(across):
        for shift in range(1, broad):
            slab_y(level, shift).wait_send()
        for column in range(broad):
            slab_core(level, column).wait_send()
    for shift in range(1, count):
        remote_done(me, lax.rem(me + shift, count)).wait_send()


def on_device(tokens, w_query, w_key, w_value, w_output, qk_gain, decay_sums):
    own_rows, decay_rows = tokens[0], decay_sums[0]
    count, groups = lax.axis_size("sp"), lax.axis_size("dp")
    tall, broad, across = layout(count, groups)
    rows, depth = own_rows.shape
    part = w_query.shape[0]
    heads, width = decay_rows.shape[0], qk_gain.shape[1]
    wide, length, block = heads * width, count * rows, 2 * rows
    tall_slab, columns = w_output.shape
    bf16, sem, chunks = jnp.bfloat16, pltpu.SemaphoreType.DMA, heads + 1
    others, beside = max(broad - 1, 1), max(across - 1, 1)
    result = pl.pallas_call(
        functools.partial(layer_kernel, heads, width, count, groups),
        out_shape=jax.ShapeDtypeStruct((rows, depth), bf16),
        in_specs=[pl.BlockSpec(memory_space=pltpu.VMEM)] * 7,
        out_specs=pl.BlockSpec(memory_space=pltpu.VMEM),
        scratch_shapes=[
            pltpu.VMEM((others, rows, depth), bf16),
            pltpu.VMEM((heads, tall, groups, part, 2 * width), bf16),
            pltpu.VMEM((tall, groups, part, wide), bf16),
            pltpu.VMEM((groups, broad, tall * tall_slab, columns), bf16),
            pltpu.VMEM((heads, broad, tall, rows, 2 * width), bf16),
            pltpu.VMEM((broad, tall, rows, wide), bf16),
            pltpu.VMEM((heads, length, 2 * width), bf16),
            pltpu.VMEM((length, wide), bf16),
            pltpu.VMEM((heads, length, 2 * width), bf16),
            pltpu.VMEM((heads, length // block, width + 16, block), bf16),
            pltpu.VMEM((count, rows, wide), bf16),
            pltpu.VMEM((count, rows, wide), bf16),
            sem((others,)), sem((others,)),
            sem((chunks, tall, 2)), sem((chunks, tall, beside)), sem((chunks, tall, across)),
            sem((chunks, tall, groups)),
            sem((chunks, broad, tall)), sem((chunks, count)),
            sem((tall, 2)), sem((tall,)), sem((across, others)), sem((across, broad)),
            sem((beside,)), sem((across,)), sem((across, broad)), sem((across, broad)),
            sem((count,)), sem((count,)),
        ],
        compiler_params=pltpu.CompilerParams(
            collective_id=0, has_side_effects=True, vmem_limit_bytes=60 * 1024 * 1024
        ),
    )(own_rows, w_query, w_key, w_value, w_output, qk_gain, decay_rows)
    return result[None]


def solution(mesh):
    placed = (
        P("dp", "sp", None),
        P("dp", "sp"),
        P("dp", "sp"),
        P("dp", "sp"),
        P("sp", "dp"),
        P(),
        P("dp", "sp", None),
    )
    return jax.shard_map(
        on_device, mesh=mesh, in_specs=placed, out_specs=P("dp", "sp", None), check_vma=False
    )
```

```python
import functools

import jax
import jax.numpy as jnp
from jax import lax
from jax.experimental import pallas as pl
from jax.experimental.pallas import tpu as pltpu
from jax.sharding import PartitionSpec as P

EPS = 1e-06
DIMS_NT = (((1,), (1,)), ((), ()))
MESH = pl.DeviceIdType.MESH
CORES = 2


def layout(count, groups):
    tall = 4 if count % 4 == 0 else 1
    return tall, count // tall, groups // CORES


def layer_kernel(
    heads, width, count, groups,
    own_ref, wq_ref, wk_ref, wv_ref, slab_ref, gain_ref, decay_ref, out_ref,
    far_ref, weight_ref, slabs_ref, stage_ref, full_ref, key_ref, value_ref, home_decay_ref,
    near_stage_ref, near_ref, done_ref, merged_ref,
    far_send, far_recv, wz_send, wx_send, wc_send, w_recv, move_send, move_recv,
    sz_send, sz_recv, sy_send, sy_recv, sx_send, sx_recv, sc_send, sc_recv, done_send, done_recv,
    near_send, near_recv, decay_send, decay_recv,
):
    rows, depth = own_ref.shape
    part = wq_ref.shape[0]
    wide = heads * width
    tall, broad, across = layout(count, groups)
    block = broad * rows
    span = wide + 16
    me, group = lax.axis_index("sp"), lax.axis_index("dp")
    z, y = me // broad, lax.rem(me, broad)
    x, core = group // CORES, lax.rem(group, CORES)
    partner = x * CORES + 1 - core

    def plane(shift):
        return lax.rem(z + shift, tall)

    def along_x(shift):
        return lax.rem(x + shift, across)

    def along_y(shift):
        return lax.rem(y + shift, broad)

    barrier = pltpu.get_barrier_semaphore()
    for shift in range(1, count):
        other = lax.rem(me + shift, count)
        pl.semaphore_signal(barrier, inc=1, device_id={"sp": other}, device_id_type=MESH)
    for shift in range(1, groups):
        peer = lax.rem(group + shift, groups)
        pl.semaphore_signal(barrier, inc=1, device_id={"dp": peer}, device_id_type=MESH)
    pl.semaphore_wait(barrier, count + groups - 2)

    def remote(source, target, out_sem, in_sem, device):
        return pltpu.make_async_remote_copy(
            src_ref=source, dst_ref=target, send_sem=out_sem, recv_sem=in_sem,
            device_id=device, device_id_type=MESH,
        )

    tokens = [
        remote(
            own_ref, far_ref.at[broad - shift - 1], far_send.at[shift - 1],
            far_recv.at[broad - shift - 1], {"sp": z * broad + along_y(shift)},
        )
        for shift in range(1, broad)
    ]

    chunks = (wk_ref, wv_ref, wq_ref)
    weights = [weight_ref.at[number] for number in range(3)]

    def weight(number, level, owner, out_sem, device):
        piece = weights[number].at[level, owner]
        return remote(piece, piece, out_sem, w_recv.at[number, level, owner], device)

    def up(number, level):
        return weight(
            number, level, group, wz_send.at[number, level, 0], {"sp": (z + 1) * broad + y}
        )

    def down(number, level):
        return weight(
            number, level, group, wz_send.at[number, level, 1], {"sp": (z - 1) * broad + y}
        )

    def sideways(number, level):
        return [
            weight(
                number, level, group, wx_send.at[number, level, shift - 1],
                {"dp": along_x(shift) * CORES + core},
            )
            for shift in range(1, across)
        ]

    def to_core(number, level, column):
        return weight(
            number, level, column * CORES + core, wc_send.at[number, level, column],
            {"dp": partner},
        )

    def own_along_z(number):
        @pl.when(z + 1 < tall)
        def _():
            up(number, z).start()

        @pl.when(z > 0)
        def _():
            down(number, z).start()

    def spread(number, level):
        for copy in sideways(number, level):
            copy.start()
        to_core(number, level, x).start()

    def relay(number, distance, onward=True, across_too=True):
        for way, step in enumerate((up, down)):
            level = z - distance if way == 0 else z + distance
            inside = (level >= 0) if way == 0 else (level < tall)
            more = (z + 1 < tall) if way == 0 else (z > 0)

            @pl.when(inside)
            def _():
                if onward:
                    step(number, level).wait_recv()

                    @pl.when(more)
                    def _():
                        step(number, level).start()

                if across_too:
                    spread(number, level)

    def relay_core(number):
        for turn in range(tall):
            for shift in range(1, across):
                level, column = plane(turn), along_x(shift)
                copy = to_core(number, level, column)
                weight(
                    number, level, column * CORES + core, wc_send.at[number, level, column],
                    {"dp": partner},
                ).wait_recv()
                copy.start()

    def gathered(number):
        for turn in range(tall):
            for column in range(across):
                level = plane(turn)
                weight(
                    number, level, column * CORES + 1 - core, wc_send.at[number, level, column],
                    {"dp": partner},
                ).wait_recv()

    def weights_sent(number):
        for turn in range(tall):
            level = plane(turn)

            @pl.when((level <= z) & (z + 1 < tall))
            def _():
                up(number, level).wait_send()

            @pl.when((level >= z) & (z > 0))
            def _():
                down(number, level).wait_send()

            for copy in sideways(number, level):
                copy.wait_send()
            for column in range(across):
                to_core(number, level, column).wait_send()

    def home_decay(turn):
        place = pl.ds(pl.multiple_of(plane(turn) * block, block), block)
        return remote(
            decay_ref.at[:, place], home_decay_ref.at[z], decay_send.at[turn], decay_recv.at[z],
            {"sp": plane(turn) * broad + y},
        )

    lane = lax.broadcasted_iota(jnp.int32, (rows, wide), 1)

    def unit(values, gain):
        values = values.astype(jnp.bfloat16).astype(jnp.float32)
        squares = values * values
        scale = jnp.zeros_like(values)
        for head in range(heads):
            inside = (lane >= head * width) & (lane < (head + 1) * width)
            total = jnp.sum(jnp.where(inside, squares, 0.0), axis=-1, keepdims=True)
            scale = jnp.where(inside, lax.rsqrt(total / width + EPS), scale)
        gains = jnp.concatenate([gain] * heads, axis=1)
        return values * scale * gains

    def row_place(source):
        return pl.ds(pl.multiple_of(source * rows, rows), rows)

    def move(number, turn, side):
        column = along_y(side)
        source = z * broad + column
        return remote(
            stage_ref.at[number, turn, row_place(column)],
            full_ref.at[number, row_place(source)],
            move_send.at[number, side, turn], move_recv.at[number, source],
            {"sp": plane(turn) * broad + y},
        )

    def needed(number, level):
        return (level > 0) if number == 2 else (level < tall - 1)

    turns = sorted(range(tall), key=lambda turn: (turn == 0, turn != tall // 2))

    def project(number, side):
        values = own_ref[...] if side == 0 else far_ref[side - 1]
        bunch = 2 if wide % 128 == 0 and tall % 2 == 0 else 1
        for first in range(0, tall, bunch):
            some = turns[first : first + bunch]
            columns = [weights[number][plane(turn)].reshape(depth, wide) for turn in some]
            result = jnp.dot(
                values, columns[0] if bunch == 1 else jnp.concatenate(columns, axis=1),
                preferred_element_type=jnp.float32,
            )
            for index, turn in enumerate(some):
                piece = result[:, index * wide : (index + 1) * wide]
                if number == 0:
                    piece = unit(piece, gain_ref[1:2, :])
                elif number == 2:
                    piece = unit(piece, gain_ref[0:1, :]) * width ** (-0.5)
                piece = piece.astype(jnp.bfloat16)
                stage_ref[number, turn, row_place(along_y(side)), :] = piece
                if turn == 0:
                    full_ref[number, row_place(z * broad + along_y(side)), :] = piece
            for turn in some:
                if turn:
                    @pl.when(needed(number, z))
                    def _():
                        move(number, turn, side).start()

    def moved(number):
        for turn in range(1, tall):
            @pl.when(needed(number, plane(turn)))
            def _():
                for column in range(broad):
                    source = plane(turn) * broad + column
                    target = full_ref.at[number, row_place(source)]
                    remote(
                        target, target, move_send.at[number, 0, turn],
                        move_recv.at[number, source], {"sp": source},
                    ).wait_recv()

    tall_slab = slab_ref.shape[0]

    def slab_z(level, way):
        place = pl.ds(pl.multiple_of(level * tall_slab, tall_slab), tall_slab)
        piece = slabs_ref.at[group, y, place]
        return remote(
            piece, piece, sz_send.at[level, way], sz_recv.at[level],
            {"sp": (z + 1 - 2 * way) * broad + y},
        )

    def slab_relay(distance):
        for way in range(2):
            level = z - distance if way == 0 else z + distance
            inside = (level >= 0) if way == 0 else (level < tall)
            onward = (z + 1 < tall) if way == 0 else (z > 0)
            if distance:
                @pl.when(inside)
                def _():
                    slab_z(level, way).wait_recv()

            @pl.when(inside & onward)
            def _():
                slab_z(level, way).start()

    def slab_x(shift):
        piece = slabs_ref.at[group, y]
        return remote(
            piece, piece, sx_send.at[shift - 1], sx_recv.at[x],
            {"dp": along_x(shift) * CORES + core},
        )

    def slab_y(level, shift):
        piece = slabs_ref.at[level * CORES + core, y]
        return remote(
            piece, piece, sy_send.at[level, shift - 1], sy_recv.at[level, y],
            {"sp": z * broad + along_y(shift)},
        )

    def slab_core(level, column):
        piece = slabs_ref.at[level * CORES + core, column]
        return remote(
            piece, piece, sc_send.at[level, column], sc_recv.at[level, column], {"dp": partner}
        )

    def slab_spread(level):
        for shift in range(1, broad):
            slab_y(level, shift).start()
        slab_core(level, y).start()

    def slabs_of_y():
        for shift in range(1, across):
            slab_x(shift).start()
        slab_spread(x)

    def slabs_from_x():
        for shift in range(1, across):
            level = along_x(shift)
            piece = slabs_ref.at[level * CORES + core, y]
            remote(
                piece, piece, sx_send.at[shift - 1], sx_recv.at[level], {"dp": group}
            ).wait_recv()
            slab_spread(level)

    def slabs_from_y():
        for turn in range(across):
            level = along_x(turn)
            for shift in range(1, broad):
                column = along_y(shift)
                piece = slabs_ref.at[level * CORES + core, column]
                remote(
                    piece, piece, sy_send.at[level, shift - 1], sy_recv.at[level, column],
                    {"sp": me},
                ).wait_recv()
                slab_core(level, column).start()

    def slabs_from_core():
        for level in range(across):
            for column in range(broad):
                piece = slabs_ref.at[level * CORES + 1 - core, column]
                remote(
                    piece, piece, sc_send.at[level, column], sc_recv.at[level, column],
                    {"dp": partner},
                ).wait_recv()

    for turn in range(1, tall):
        home_decay(turn).start()
    home_decay_ref[z] = decay_ref[:, pl.ds(pl.multiple_of(z * block, block), block)]
    for number in range(3):
        weight_ref[number, z, group] = chunks[number][...]
        if number < 2:
            own_along_z(number)
            spread(number, z)
        if number == 0:
            for copy in tokens:
                copy.start()
    slabs_ref[group, y, pl.ds(pl.multiple_of(z * tall_slab, tall_slab), tall_slab), :] = slab_ref[
        ...
    ]

    def ready(number):
        relay_core(number)
        gathered(number)

    rest = (2,)
    for distance in range(1, tall):
        relay(0, distance)
        if distance == 1:
            relay(1, 1, across_too=False)
            for number in rest:
                own_along_z(number)
        elif distance == 2:
            relay(1, 1, onward=False)
            relay(1, 2, across_too=False)
    for number in rest:
        relay(number, 1, across_too=False)
    if tall > 2:
        relay(1, 2, onward=False)
    ready(0)
    for distance in range(3, tall):
        relay(1, distance)
    project(0, 0)
    for number in rest:
        spread(number, z)
        relay(number, 1, onward=False)
        if tall > 2:
            relay(number, 2)
    ready(1)
    for number in rest:
        for distance in range(3, tall):
            relay(number, distance)
    project(1, 0)
    slab_relay(0)
    for copy in tokens:
        copy.wait_recv()
    for number in range(2):
        for side in range(1, broad):
            project(number, side)
    for distance in range(1, tall):
        slab_relay(distance)
    for number in rest:
        ready(number)
        for side in range(broad):
            project(number, side)

    def split(values):
        first = values.astype(jnp.bfloat16).astype(jnp.float32)
        rest = values - first
        second = rest.astype(jnp.bfloat16).astype(jnp.float32)
        return first, second, rest - second

    block_lane = lax.broadcasted_iota(jnp.int32, (block, 2 * width), 1)
    ones_rows = jnp.where(lax.broadcasted_iota(jnp.int32, (16, block), 0) == 0, 1.0, 0.0)
    packed = wide == 2 * width

    def aside(head):
        return width if packed and head == 0 else 0

    def beside(head):
        low = aside(head)
        return (block_lane >= low) & (block_lane < low + width)

    def with_lanes(values, head, lanes):
        if packed:
            return jnp.where(beside(head), lanes, values.astype(jnp.float32)).astype(jnp.bfloat16)
        own = values[:, head * width : (head + 1) * width].astype(jnp.float32)
        return jnp.concatenate([lanes[:, :width], own], axis=1).astype(jnp.bfloat16)

    def query_operand(values, head):
        low = aside(head)
        ones = jnp.where((block_lane >= low) & (block_lane < low + 3), 1.0, 0.0)
        return with_lanes(values, head, ones)

    def key_operands(values, decay):
        sub = lax.broadcasted_iota(jnp.int32, (2 * width, block), 0)
        lanes = jnp.zeros((2 * width, block), jnp.float32)
        fresh = []
        for head in range(heads):
            for index, piece in enumerate(split(-decay[head : head + 1, :])):
                lanes = jnp.where(sub == aside(head) + index, piece, lanes)
            if not packed:
                fresh.append(with_lanes(values, head, lanes.T))
        if packed:
            turned = lanes.T
            fresh = [with_lanes(values, head, turned) for head in range(heads)]
        return fresh

    def value_operands(values):
        turned = values.astype(jnp.float32).T
        return [
            jnp.concatenate(
                [turned[head * width : (head + 1) * width], ones_rows], axis=0
            ).astype(jnp.bfloat16)
            for head in range(heads)
        ]

    def finish(parts):
        mixed, logs = [], []
        for peak, total in parts:
            norm = total[width : width + 1]
            mixed.append(total[:width] / norm)
            logs.extend(split(peak + jnp.log(norm)))
        sub = lax.broadcasted_iota(jnp.int32, (16, block), 0)
        tail = jnp.zeros((16, block), jnp.float32)
        for index, piece in enumerate(logs):
            tail = jnp.where(sub == index, piece, tail)
        result = jnp.concatenate([*mixed, tail], axis=0)
        return [
            (pltpu.roll(result, block - column * rows, 1) if column else result)[
                :, :rows
            ].astype(jnp.bfloat16)
            for column in range(broad)
        ]

    def scores_of(keys, queries):
        return lax.dot_general(keys, queries, DIMS_NT, preferred_element_type=jnp.float32)

    def near_copy(turn, side):
        column = along_y(side)
        return remote(
            near_stage_ref.at[turn, column], near_ref.at[plane(turn) * broad + y],
            near_send.at[turn, side], near_recv.at[plane(turn) * broad + y],
            {"sp": z * broad + column},
        )

    key_place = lax.broadcasted_iota(jnp.int32, (block, block), 0)
    query_place = lax.broadcasted_iota(jnp.int32, (block, block), 1)

    def near_block(turn, unused):
        keys = key_operands(stage_ref[0, turn], home_decay_ref[plane(turn)])
        values = value_operands(stage_ref[1, turn])
        parts = []
        for head in range(heads):
            scores = scores_of(keys[head], query_operand(stage_ref[2, turn], head))
            scores = jnp.where(key_place <= query_place, scores, -jnp.inf)
            peak = jnp.max(scores, axis=0, keepdims=True)
            probs = jnp.exp(scores - peak).astype(jnp.bfloat16)
            parts.append(
                (peak, jnp.dot(values[head], probs, preferred_element_type=jnp.float32))
            )
        for column, piece in enumerate(finish(parts)):
            near_stage_ref[turn, column] = piece
        near_ref[plane(turn) * broad + y] = near_stage_ref[turn, y]
        for side in range(1, broad):
            near_copy(turn, side).start()

        @pl.when(turn == 0)
        def _():
            slabs_of_y()

        @pl.when(turn == 2)
        def _():
            slabs_from_x()

        return unused

    for turn in range(1, tall):
        remote(
            home_decay_ref.at[plane(turn)], home_decay_ref.at[plane(turn)], decay_send.at[turn],
            decay_recv.at[plane(turn)], {"sp": me},
        ).wait_recv()
    lax.fori_loop(0, tall, near_block, 0)

    moved(0)
    moved(1)

    def prepare(level, unused):
        place = pl.ds(pl.multiple_of(level * block, block), block)
        keys = key_operands(full_ref[0, place, :], decay_ref[:, place])
        values = value_operands(full_ref[1, place, :])
        for head in range(heads):
            key_ref[head, level] = keys[head]
            value_ref[head, level] = values[head]
        return unused

    lax.fori_loop(0, tall - 1, prepare, 0)
    moved(2)

    def remote_done(level, column):
        owner = level * broad + column
        return remote(
            done_ref.at[level, column], merged_ref.at[me], done_send.at[level, column],
            done_recv.at[me], {"sp": owner},
        )

    def far_block(index, unused):
        level = tall - 1 - index
        place = pl.ds(pl.multiple_of(level * block, block), block)
        queries = [query_operand(full_ref[2, place, :], head) for head in range(heads)]

        def step(column, carry):
            fresh = []
            for head in range(heads):
                peak, total = carry[head]
                scores = scores_of(key_ref[head, column], queries[head])
                higher = jnp.maximum(peak, jnp.max(scores, axis=0, keepdims=True))
                probs = jnp.exp(scores - higher).astype(jnp.bfloat16)
                total = total * jnp.exp(peak - higher) + jnp.dot(
                    value_ref[head, column], probs, preferred_element_type=jnp.float32
                )
                fresh.append((higher, total))
            return tuple(fresh)

        start = tuple(
            (
                jnp.full((1, block), -1e30, jnp.float32),
                jnp.zeros((width + 16, block), jnp.float32),
            )
            for _ in range(heads)
        )
        carry = lax.fori_loop(0, level, step, start)
        for column, piece in enumerate(finish(carry)):
            done_ref[level, column] = piece

            @pl.when(level * broad + column != me)
            def _():
                remote_done(level, column).start()

        @pl.when(index == 0)
        def _():
            slabs_from_y()

        return unused

    lax.fori_loop(0, tall - 1, far_block, 0)

    @pl.when(z > 0)
    def _():
        merged_ref[me] = done_ref[z, y]
        for shift in range(1, count):
            source = lax.rem(me + shift, count)
            target = merged_ref.at[source]
            remote(
                target, target, done_send.at[0, 0], done_recv.at[source], {"sp": source}
            ).wait_recv()

    @pl.when(z == 0)
    def _():
        nothing = jnp.where(
            lax.broadcasted_iota(jnp.int32, (span, rows), 0) < wide, 0.0, -1e30
        ).astype(jnp.bfloat16)
        for source in range(count):
            merged_ref[source] = nothing

    for turn in range(tall):
        for side in range(1, broad):
            target = near_ref.at[plane(turn) * broad + along_y(side)]
            remote(
                target, target, near_send.at[turn, side],
                near_recv.at[plane(turn) * broad + along_y(side)], {"sp": me},
            ).wait_recv()
    slabs_from_core()

    def combined(source):
        one, two = (ref[source].astype(jnp.float32) for ref in (near_ref, merged_ref))
        outs = []
        for head in range(heads):
            low = wide + 3 * head
            logs = [sum(part[low + i : low + i + 1] for i in range(3)) for part in (one, two)]
            peak = jnp.maximum(*logs)
            first, second = (jnp.exp(log - peak) for log in logs)
            norm = first + second
            place = slice(head * width, (head + 1) * width)
            mixed = one[place] * (first / norm) + two[place] * (second / norm)
            scale = lax.rsqrt(jnp.mean(mixed * mixed, axis=0, keepdims=True) + EPS)
            outs.append(mixed * scale)
        return jnp.concatenate(outs, axis=0).T.astype(jnp.bfloat16)

    merged = jnp.concatenate(
        [combined(level * broad + column) for column in range(broad) for level in range(tall)],
        axis=1,
    )
    columns = slab_ref.shape[1]
    for place in range(groups):
        out_ref[:, place * columns : (place + 1) * columns] = jnp.dot(
            merged, slabs_ref[place].reshape(-1, columns), preferred_element_type=jnp.float32
        ).astype(out_ref.dtype)

    for copy in tokens:
        copy.wait_send()
    for number in range(3):
        weights_sent(number)

        @pl.when(needed(number, z))
        def _():
            for side in range(broad):
                for turn in range(1, tall):
                    move(number, turn, side).wait_send()
    for turn in range(tall):
        if turn:
            home_decay(turn).wait_send()
        for side in range(1, broad):
            near_copy(turn, side).wait_send()
    for distance in range(tall):
        for way in range(2):
            level = z - distance if way == 0 else z + distance
            inside = (level >= 0) if way == 0 else (level < tall)
            onward = (z + 1 < tall) if way == 0 else (z > 0)

            @pl.when(inside & onward)
            def _():
                slab_z(level, way).wait_send()

    for shift in range(1, across):
        slab_x(shift).wait_send()
    for level in range(across):
        for shift in range(1, broad):
            slab_y(level, shift).wait_send()
        for column in range(broad):
            slab_core(level, column).wait_send()
    for level in range(1, tall):
        for column in range(broad):
            @pl.when(level * broad + column != me)
            def _():
                remote_done(level, column).wait_send()


def on_device(tokens, w_query, w_key, w_value, w_output, qk_gain, decay_sums):
    own_rows, decay_rows = tokens[0], decay_sums[0]
    count, groups = lax.axis_size("sp"), lax.axis_size("dp")
    tall, broad, across = layout(count, groups)
    rows, depth = own_rows.shape
    part = w_query.shape[0]
    heads, width = decay_rows.shape[0], qk_gain.shape[1]
    wide, length, block = heads * width, count * rows, broad * rows
    tall_slab, columns = w_output.shape
    bf16, sem, span = jnp.bfloat16, pltpu.SemaphoreType.DMA, wide + 16
    others, beside = max(broad - 1, 1), max(across - 1, 1)
    result = pl.pallas_call(
        functools.partial(layer_kernel, heads, width, count, groups),
        out_shape=jax.ShapeDtypeStruct((rows, depth), bf16),
        in_specs=[pl.BlockSpec(memory_space=pltpu.VMEM)] * 7,
        out_specs=pl.BlockSpec(memory_space=pltpu.VMEM),
        scratch_shapes=[
            pltpu.VMEM((others, rows, depth), bf16),
            pltpu.VMEM((3, tall, groups, part, wide), bf16),
            pltpu.VMEM((groups, broad, tall * tall_slab, columns), bf16),
            pltpu.VMEM((3, tall, block, wide), bf16),
            pltpu.VMEM((3, length, wide), bf16),
            pltpu.VMEM((heads, tall, block, 2 * width), bf16),
            pltpu.VMEM((heads, tall, width + 16, block), bf16),
            pltpu.VMEM((tall, heads, block), jnp.float32),
            pltpu.VMEM((tall, broad, span, rows), bf16),
            pltpu.VMEM((count, span, rows), bf16),
            pltpu.VMEM((tall, broad, span, rows), bf16),
            pltpu.VMEM((count, span, rows), bf16),
            sem((others,)), sem((others,)),
            sem((3, tall, 2)), sem((3, tall, beside)), sem((3, tall, across)),
            sem((3, tall, groups)),
            sem((3, broad, tall)), sem((3, count)),
            sem((tall, 2)), sem((tall,)), sem((across, others)), sem((across, broad)),
            sem((beside,)), sem((across,)), sem((across, broad)), sem((across, broad)),
            sem((tall, broad)), sem((count,)),
            sem((tall, broad)), sem((count,)), sem((tall,)), sem((tall,)),
        ],
        compiler_params=pltpu.CompilerParams(
            collective_id=0, has_side_effects=True, vmem_limit_bytes=60 * 1024 * 1024
        ),
    )(own_rows, w_query, w_key, w_value, w_output, qk_gain, decay_rows)
    return result[None]


def solution(mesh):
    placed = (
        P("dp", "sp", None),
        P("dp", "sp"),
        P("dp", "sp"),
        P("dp", "sp"),
        P("sp", "dp"),
        P(),
        P("dp", "sp", None),
    )
    return jax.shard_map(
        on_device, mesh=mesh, in_specs=placed, out_specs=P("dp", "sp", None), check_vma=False
    )
```

```python
import functools

import jax
import jax.numpy as jnp
from jax import lax
from jax.experimental import pallas as pl
from jax.experimental.pallas import tpu as pltpu
from jax.sharding import PartitionSpec as P

EPS = 1e-06
DIMS_NT = (((1,), (1,)), ((), ()))
MESH = pl.DeviceIdType.MESH
CORES = 2


def layout(count, groups):
    tall = 4 if count % 4 == 0 else 1
    return tall, count // tall, groups // CORES


def layer_kernel(
    heads, width, count, groups,
    own_ref, wq_ref, wk_ref, wv_ref, slab_ref, gain_ref, decay_ref, out_ref,
    far_ref, weight_ref, slabs_ref, stage_ref, full_ref, key_ref, value_ref, home_decay_ref,
    near_stage_ref, near_ref, done_ref, merged_ref, log_ref, logs_ref,
    far_send, far_recv, wz_send, wx_send, wc_send, w_recv, move_send, move_recv,
    sz_send, sz_recv, sy_send, sy_recv, sx_send, sx_recv, sc_send, sc_recv, done_send, done_recv,
    near_send, near_recv, decay_send, decay_recv, log_send, log_recv,
):
    rows, depth = own_ref.shape
    part = wq_ref.shape[0]
    wide = heads * width
    tall, broad, across = layout(count, groups)
    block = broad * rows
    span = wide + 16
    me, group = lax.axis_index("sp"), lax.axis_index("dp")
    z, y = me // broad, lax.rem(me, broad)
    x, core = group // CORES, lax.rem(group, CORES)
    partner = x * CORES + 1 - core

    def plane(shift):
        return lax.rem(z + shift, tall)

    def along_x(shift):
        return lax.rem(x + shift, across)

    def along_y(shift):
        return lax.rem(y + shift, broad)

    barrier = pltpu.get_barrier_semaphore()
    for shift in range(1, count):
        other = lax.rem(me + shift, count)
        pl.semaphore_signal(barrier, inc=1, device_id={"sp": other}, device_id_type=MESH)
    for shift in range(1, groups):
        peer = lax.rem(group + shift, groups)
        pl.semaphore_signal(barrier, inc=1, device_id={"dp": peer}, device_id_type=MESH)
    pl.semaphore_wait(barrier, count + groups - 2)

    def remote(source, target, out_sem, in_sem, device):
        return pltpu.make_async_remote_copy(
            src_ref=source, dst_ref=target, send_sem=out_sem, recv_sem=in_sem,
            device_id=device, device_id_type=MESH,
        )

    tokens = [
        remote(
            own_ref, far_ref.at[broad - shift - 1], far_send.at[shift - 1],
            far_recv.at[broad - shift - 1], {"sp": z * broad + along_y(shift)},
        )
        for shift in range(1, broad)
    ]

    chunks = (wk_ref, wv_ref, wq_ref)
    weights = [weight_ref.at[number] for number in range(3)]

    def weight(number, level, owner, out_sem, device):
        piece = weights[number].at[level, owner]
        return remote(piece, piece, out_sem, w_recv.at[number, level, owner], device)

    def up(number, level):
        return weight(
            number, level, group, wz_send.at[number, level, 0], {"sp": (z + 1) * broad + y}
        )

    def down(number, level):
        return weight(
            number, level, group, wz_send.at[number, level, 1], {"sp": (z - 1) * broad + y}
        )

    def sideways(number, level):
        return [
            weight(
                number, level, group, wx_send.at[number, level, shift - 1],
                {"dp": along_x(shift) * CORES + core},
            )
            for shift in range(1, across)
        ]

    def to_core(number, level, column):
        return weight(
            number, level, column * CORES + core, wc_send.at[number, level, column],
            {"dp": partner},
        )

    def own_along_z(number):
        @pl.when(z + 1 < tall)
        def _():
            up(number, z).start()

        @pl.when(z > 0)
        def _():
            down(number, z).start()

    def spread(number, level):
        for copy in sideways(number, level):
            copy.start()
        to_core(number, level, x).start()

    def relay(number, distance, onward=True, across_too=True):
        for way, step in enumerate((up, down)):
            level = z - distance if way == 0 else z + distance
            inside = (level >= 0) if way == 0 else (level < tall)
            more = (z + 1 < tall) if way == 0 else (z > 0)

            @pl.when(inside)
            def _():
                if onward:
                    step(number, level).wait_recv()

                    @pl.when(more)
                    def _():
                        step(number, level).start()

                if across_too:
                    spread(number, level)

    def relay_core(number):
        for turn in range(tall):
            for shift in range(1, across):
                level, column = plane(turn), along_x(shift)
                copy = to_core(number, level, column)
                weight(
                    number, level, column * CORES + core, wc_send.at[number, level, column],
                    {"dp": partner},
                ).wait_recv()
                copy.start()

    def gathered(number):
        for turn in range(tall):
            for column in range(across):
                level = plane(turn)
                weight(
                    number, level, column * CORES + 1 - core, wc_send.at[number, level, column],
                    {"dp": partner},
                ).wait_recv()

    def weights_sent(number):
        for turn in range(tall):
            level = plane(turn)

            @pl.when((level <= z) & (z + 1 < tall))
            def _():
                up(number, level).wait_send()

            @pl.when((level >= z) & (z > 0))
            def _():
                down(number, level).wait_send()

            for copy in sideways(number, level):
                copy.wait_send()
            for column in range(across):
                to_core(number, level, column).wait_send()

    def home_decay(turn):
        place = pl.ds(pl.multiple_of(plane(turn) * block, block), block)
        return remote(
            decay_ref.at[:, place], home_decay_ref.at[z], decay_send.at[turn], decay_recv.at[z],
            {"sp": plane(turn) * broad + y},
        )

    lane = lax.broadcasted_iota(jnp.int32, (rows, wide), 1)

    def unit(values, gain):
        values = values.astype(jnp.bfloat16).astype(jnp.float32)
        squares = values * values
        scale = jnp.zeros_like(values)
        for head in range(heads):
            inside = (lane >= head * width) & (lane < (head + 1) * width)
            total = jnp.sum(jnp.where(inside, squares, 0.0), axis=-1, keepdims=True)
            scale = jnp.where(inside, lax.rsqrt(total / width + EPS), scale)
        gains = jnp.concatenate([gain] * heads, axis=1)
        return values * scale * gains

    def row_place(source):
        return pl.ds(pl.multiple_of(source * rows, rows), rows)

    def move(number, turn, side):
        column = along_y(side)
        source = z * broad + column
        return remote(
            stage_ref.at[number, turn, row_place(column)],
            full_ref.at[number, row_place(source)],
            move_send.at[number, side, turn], move_recv.at[number, source],
            {"sp": plane(turn) * broad + y},
        )

    def needed(number, level):
        return (level > 0) if number == 2 else (level < tall - 1)

    turns = sorted(range(tall), key=lambda turn: (turn == 0, turn != tall // 2))

    def project(number, side):
        values = own_ref[...] if side == 0 else far_ref[side - 1]
        bunch = 2 if wide % 128 == 0 and tall % 2 == 0 else 1
        for first in range(0, tall, bunch):
            some = turns[first : first + bunch]
            columns = [weights[number][plane(turn)].reshape(depth, wide) for turn in some]
            result = jnp.dot(
                values, columns[0] if bunch == 1 else jnp.concatenate(columns, axis=1),
                preferred_element_type=jnp.float32,
            )
            for index, turn in enumerate(some):
                piece = result[:, index * wide : (index + 1) * wide]
                if number == 0:
                    piece = unit(piece, gain_ref[1:2, :])
                elif number == 2:
                    piece = unit(piece, gain_ref[0:1, :]) * width ** (-0.5)
                piece = piece.astype(jnp.bfloat16)
                stage_ref[number, turn, row_place(along_y(side)), :] = piece
                if turn == 0:
                    full_ref[number, row_place(z * broad + along_y(side)), :] = piece
            for turn in some:
                if turn:
                    @pl.when(needed(number, z))
                    def _():
                        move(number, turn, side).start()

    def moved(number, level):
        @pl.when((level != z) & needed(number, level))
        def _():
            for column in range(broad):
                source = level * broad + column
                target = full_ref.at[number, row_place(source)]
                remote(
                    target, target, move_send.at[number, 0, 0], move_recv.at[number, source],
                    {"sp": source},
                ).wait_recv()

    tall_slab = slab_ref.shape[0]

    def slab_z(level, way):
        place = pl.ds(pl.multiple_of(level * tall_slab, tall_slab), tall_slab)
        piece = slabs_ref.at[group, y, place]
        return remote(
            piece, piece, sz_send.at[level, way], sz_recv.at[level],
            {"sp": (z + 1 - 2 * way) * broad + y},
        )

    def slab_relay(distance):
        for way in range(2):
            level = z - distance if way == 0 else z + distance
            inside = (level >= 0) if way == 0 else (level < tall)
            onward = (z + 1 < tall) if way == 0 else (z > 0)
            if distance:
                @pl.when(inside)
                def _():
                    slab_z(level, way).wait_recv()

            @pl.when(inside & onward)
            def _():
                slab_z(level, way).start()

    def slab_y(shift):
        piece = slabs_ref.at[group, y]
        return remote(
            piece, piece, sy_send.at[shift - 1], sy_recv.at[y],
            {"sp": z * broad + along_y(shift)},
        )

    def slab_x(column, shift):
        piece = slabs_ref.at[group, column]
        return remote(
            piece, piece, sx_send.at[column, shift - 1], sx_recv.at[x, column],
            {"dp": along_x(shift) * CORES + core},
        )

    def slab_core(level, column):
        piece = slabs_ref.at[level * CORES + core, column]
        return remote(
            piece, piece, sc_send.at[level, column], sc_recv.at[level, column], {"dp": partner}
        )

    def slab_spread(column):
        for shift in range(1, across):
            slab_x(column, shift).start()
        slab_core(x, column).start()

    def slabs_of_z():
        for shift in range(1, broad):
            slab_y(shift).start()
        slab_spread(y)

    def slabs_from_y():
        for shift in range(1, broad):
            column = along_y(shift)
            piece = slabs_ref.at[group, column]
            remote(
                piece, piece, sy_send.at[shift - 1], sy_recv.at[column], {"sp": me}
            ).wait_recv()
            slab_spread(column)

    def slabs_from_x():
        for turn in range(broad):
            column = along_y(turn)
            for shift in range(1, across):
                level = along_x(shift)
                piece = slabs_ref.at[level * CORES + core, column]
                remote(
                    piece, piece, sx_send.at[column, shift - 1], sx_recv.at[level, column],
                    {"dp": group},
                ).wait_recv()
                slab_core(level, column).start()

    def slabs_from_core():
        for level in range(across):
            for column in range(broad):
                piece = slabs_ref.at[level * CORES + 1 - core, column]
                remote(
                    piece, piece, sc_send.at[level, column], sc_recv.at[level, column],
                    {"dp": partner},
                ).wait_recv()

    for turn in range(1, tall):
        home_decay(turn).start()
    home_decay_ref[z] = decay_ref[:, pl.ds(pl.multiple_of(z * block, block), block)]
    for number in range(3):
        weight_ref[number, z, group] = chunks[number][...]
        if number < 2:
            own_along_z(number)
            spread(number, z)
        if number == 0:
            for copy in tokens:
                copy.start()
    slabs_ref[group, y, pl.ds(pl.multiple_of(z * tall_slab, tall_slab), tall_slab), :] = slab_ref[
        ...
    ]

    def ready(number):
        relay_core(number)
        gathered(number)

    rest = (2,)
    for distance in range(1, tall):
        relay(0, distance)
        if distance == 1:
            relay(1, 1, across_too=False)
            for number in rest:
                own_along_z(number)
            slab_relay(0)
        elif distance == 2:
            relay(1, 1, onward=False)
            relay(1, 2, across_too=False)
    for number in rest:
        relay(number, 1, across_too=False)
    if tall > 2:
        relay(1, 2, onward=False)
    if tall > 1:
        slab_relay(1)
    ready(0)
    for distance in range(3, tall):
        relay(1, distance)
    project(0, 0)
    for number in rest:
        spread(number, z)
        relay(number, 1, onward=False)
        if tall > 2:
            relay(number, 2)
    if tall > 2:
        slab_relay(2)
    ready(1)
    for number in rest:
        for distance in range(3, tall):
            relay(number, distance)
    project(1, 0)
    for copy in tokens:
        copy.wait_recv()
    for number in range(2):
        for side in range(1, broad):
            project(number, side)
    for distance in range(3, tall):
        slab_relay(distance)
    slabs_of_z()
    for number in rest:
        ready(number)
        for side in range(broad):
            project(number, side)

    def split(values):
        first = values.astype(jnp.bfloat16).astype(jnp.float32)
        rest = values - first
        second = rest.astype(jnp.bfloat16).astype(jnp.float32)
        return first, second, rest - second

    block_lane = lax.broadcasted_iota(jnp.int32, (block, 2 * width), 1)
    ones_rows = jnp.where(lax.broadcasted_iota(jnp.int32, (16, block), 0) == 0, 1.0, 0.0)
    packed = wide == 2 * width

    def aside(head):
        return width if packed and head == 0 else 0

    def beside(head):
        low = aside(head)
        return (block_lane >= low) & (block_lane < low + width)

    def with_lanes(values, head, lanes):
        if packed:
            return jnp.where(beside(head), lanes, values.astype(jnp.float32)).astype(jnp.bfloat16)
        own = values[:, head * width : (head + 1) * width].astype(jnp.float32)
        return jnp.concatenate([lanes[:, :width], own], axis=1).astype(jnp.bfloat16)

    def query_operand(values, head):
        low = aside(head)
        ones = jnp.where((block_lane >= low) & (block_lane < low + 3), 1.0, 0.0)
        return with_lanes(values, head, ones)

    def key_operands(values, decay):
        sub = lax.broadcasted_iota(jnp.int32, (2 * width, block), 0)
        lanes = jnp.zeros((2 * width, block), jnp.float32)
        fresh = []
        for head in range(heads):
            for index, piece in enumerate(split(-decay[head : head + 1, :])):
                lanes = jnp.where(sub == aside(head) + index, piece, lanes)
            if not packed:
                fresh.append(with_lanes(values, head, lanes.T))
        if packed:
            turned = lanes.T
            fresh = [with_lanes(values, head, turned) for head in range(heads)]
        return fresh

    def value_operands(values):
        turned = values.astype(jnp.float32).T
        return [
            jnp.concatenate(
                [turned[head * width : (head + 1) * width], ones_rows], axis=0
            ).astype(jnp.bfloat16)
            for head in range(heads)
        ]

    def averages(parts):
        mixed, logs = [], []
        for peak, total in parts:
            norm = total[width : width + 1]
            mixed.append(total[:width] / norm)
            logs.append(peak + jnp.log(norm))
        return mixed, logs

    def pieces(values):
        return [
            (pltpu.roll(values, block - column * rows, 1) if column else values)[:, :rows]
            for column in range(broad)
        ]

    def stacked(rows_of, extent):
        sub = lax.broadcasted_iota(jnp.int32, (extent, block), 0)
        result = jnp.zeros((extent, block), jnp.float32)
        for index, piece in enumerate(rows_of):
            result = jnp.where(sub == index, piece, result)
        return result

    def scores_of(keys, queries):
        return lax.dot_general(keys, queries, DIMS_NT, preferred_element_type=jnp.float32)

    def near_copy(turn, side):
        column = along_y(side)
        return remote(
            near_stage_ref.at[turn, column], near_ref.at[plane(turn) * broad + y],
            near_send.at[turn, side], near_recv.at[plane(turn) * broad + y],
            {"sp": z * broad + column},
        )

    key_place = lax.broadcasted_iota(jnp.int32, (block, block), 0)
    query_place = lax.broadcasted_iota(jnp.int32, (block, block), 1)

    def near_block(turn, unused):
        keys = key_operands(stage_ref[0, turn], home_decay_ref[plane(turn)])
        values = value_operands(stage_ref[1, turn])
        parts = []
        for head in range(heads):
            scores = scores_of(keys[head], query_operand(stage_ref[2, turn], head))
            scores = jnp.where(key_place <= query_place, scores, -jnp.inf)
            peak = jnp.max(scores, axis=0, keepdims=True)
            probs = jnp.exp(scores - peak).astype(jnp.bfloat16)
            parts.append(
                (peak, jnp.dot(values[head], probs, preferred_element_type=jnp.float32))
            )
        mixed, logs = averages(parts)
        tail = stacked([piece for log in logs for piece in split(log)], 16)
        for column, piece in enumerate(pieces(jnp.concatenate([*mixed, tail], axis=0))):
            near_stage_ref[turn, column] = piece.astype(jnp.bfloat16)
        near_ref[plane(turn) * broad + y] = near_stage_ref[turn, y]
        for side in range(1, broad):
            near_copy(turn, side).start()

        return unused

    for turn in range(1, tall):
        remote(
            home_decay_ref.at[plane(turn)], home_decay_ref.at[plane(turn)], decay_send.at[turn],
            decay_recv.at[plane(turn)], {"sp": me},
        ).wait_recv()
    slabs_from_y()
    lax.fori_loop(0, tall, near_block, 0)

    def prepare(level, unused):
        moved(0, level)
        moved(1, level)
        place = pl.ds(pl.multiple_of(level * block, block), block)
        keys = key_operands(full_ref[0, place, :], decay_ref[:, place])
        values = value_operands(full_ref[1, place, :])
        for head in range(heads):
            key_ref[head, level] = keys[head]
            value_ref[head, level] = values[head]
        return unused

    lax.fori_loop(0, tall - 1, prepare, 0)

    def remote_done(level, column):
        device = {"sp": level * broad + column}
        return [
            remote(
                done_ref.at[level, column], merged_ref.at[me], done_send.at[level, column],
                done_recv.at[me], device,
            ),
            remote(
                log_ref.at[level, column], logs_ref.at[me], log_send.at[level, column],
                log_recv.at[me], device,
            ),
        ]

    def far_block(index, unused):
        level = tall - 1 - index
        moved(2, level)
        place = pl.ds(pl.multiple_of(level * block, block), block)
        queries = [query_operand(full_ref[2, place, :], head) for head in range(heads)]

        def step(column, carry):
            fresh = []
            for head in range(heads):
                peak, total = carry[head]
                scores = scores_of(key_ref[head, column], queries[head])
                higher = jnp.maximum(peak, jnp.max(scores, axis=0, keepdims=True))
                probs = jnp.exp(scores - higher).astype(jnp.bfloat16)
                total = total * jnp.exp(peak - higher) + jnp.dot(
                    value_ref[head, column], probs, preferred_element_type=jnp.float32
                )
                fresh.append((higher, total))
            return tuple(fresh)

        start = tuple(
            (
                jnp.full((1, block), -1e30, jnp.float32),
                jnp.zeros((width + 16, block), jnp.float32),
            )
            for _ in range(heads)
        )
        carry = lax.fori_loop(0, level, step, start)
        mixed, logs = averages(carry)
        turned = jnp.concatenate(mixed, axis=0).T.astype(jnp.bfloat16)
        for column, piece in enumerate(pieces(stacked(logs, 8))):
            log_ref[level, column] = piece
            done_ref[level, column] = turned[column * rows : (column + 1) * rows]

            @pl.when(level * broad + column != me)
            def _():
                for copy in remote_done(level, column):
                    copy.start()

        @pl.when(index == min(1, tall - 2))
        def _():
            slabs_from_x()

        return unused

    lax.fori_loop(0, tall - 1, far_block, 0)

    @pl.when(z > 0)
    def _():
        merged_ref[me] = done_ref[z, y]
        logs_ref[me] = log_ref[z, y]
        for shift in range(1, count):
            source = lax.rem(me + shift, count)
            remote(
                merged_ref.at[source], merged_ref.at[source], done_send.at[0, 0],
                done_recv.at[source], {"sp": source},
            ).wait_recv()
            remote(
                logs_ref.at[source], logs_ref.at[source], log_send.at[0, 0],
                log_recv.at[source], {"sp": source},
            ).wait_recv()

    @pl.when(z == 0)
    def _():
        for source in range(count):
            merged_ref[source] = jnp.zeros((rows, wide), jnp.bfloat16)
            logs_ref[source] = jnp.full((8, rows), -1e30, jnp.float32)

    for turn in range(tall):
        for side in range(1, broad):
            target = near_ref.at[plane(turn) * broad + along_y(side)]
            remote(
                target, target, near_send.at[turn, side],
                near_recv.at[plane(turn) * broad + along_y(side)], {"sp": me},
            ).wait_recv()
    slabs_from_core()

    def combined(source):
        one = near_ref[source].astype(jnp.float32)
        two = merged_ref[source].astype(jnp.float32).T
        outs = []
        for head in range(heads):
            low = wide + 3 * head
            near_log = sum(one[low + i : low + i + 1] for i in range(3))
            logs = near_log, logs_ref[source][head : head + 1]
            peak = jnp.maximum(*logs)
            first, second = (jnp.exp(log - peak) for log in logs)
            norm = first + second
            place = slice(head * width, (head + 1) * width)
            mixed = one[place] * (first / norm) + two[place] * (second / norm)
            scale = lax.rsqrt(jnp.mean(mixed * mixed, axis=0, keepdims=True) + EPS)
            outs.append(mixed * scale)
        return jnp.concatenate(outs, axis=0).T.astype(jnp.bfloat16)

    merged = jnp.concatenate(
        [combined(level * broad + column) for column in range(broad) for level in range(tall)],
        axis=1,
    )
    columns = slab_ref.shape[1]
    for place in range(groups):
        out_ref[:, place * columns : (place + 1) * columns] = jnp.dot(
            merged, slabs_ref[place].reshape(-1, columns), preferred_element_type=jnp.float32
        ).astype(out_ref.dtype)

    for copy in tokens:
        copy.wait_send()
    for number in range(3):
        weights_sent(number)

        @pl.when(needed(number, z))
        def _():
            for side in range(broad):
                for turn in range(1, tall):
                    move(number, turn, side).wait_send()
    for turn in range(tall):
        if turn:
            home_decay(turn).wait_send()
        for side in range(1, broad):
            near_copy(turn, side).wait_send()
    for distance in range(tall):
        for way in range(2):
            level = z - distance if way == 0 else z + distance
            inside = (level >= 0) if way == 0 else (level < tall)
            onward = (z + 1 < tall) if way == 0 else (z > 0)

            @pl.when(inside & onward)
            def _():
                slab_z(level, way).wait_send()

    for shift in range(1, broad):
        slab_y(shift).wait_send()
    for column in range(broad):
        for shift in range(1, across):
            slab_x(column, shift).wait_send()
        for level in range(across):
            slab_core(level, column).wait_send()
    for level in range(1, tall):
        for column in range(broad):
            @pl.when(level * broad + column != me)
            def _():
                for copy in remote_done(level, column):
                    copy.wait_send()


def on_device(tokens, w_query, w_key, w_value, w_output, qk_gain, decay_sums):
    own_rows, decay_rows = tokens[0], decay_sums[0]
    count, groups = lax.axis_size("sp"), lax.axis_size("dp")
    tall, broad, across = layout(count, groups)
    rows, depth = own_rows.shape
    part = w_query.shape[0]
    heads, width = decay_rows.shape[0], qk_gain.shape[1]
    wide, length, block = heads * width, count * rows, broad * rows
    tall_slab, columns = w_output.shape
    bf16, sem, span = jnp.bfloat16, pltpu.SemaphoreType.DMA, wide + 16
    others, beside = max(broad - 1, 1), max(across - 1, 1)
    result = pl.pallas_call(
        functools.partial(layer_kernel, heads, width, count, groups),
        out_shape=jax.ShapeDtypeStruct((rows, depth), bf16),
        in_specs=[pl.BlockSpec(memory_space=pltpu.VMEM)] * 7,
        out_specs=pl.BlockSpec(memory_space=pltpu.VMEM),
        scratch_shapes=[
            pltpu.VMEM((others, rows, depth), bf16),
            pltpu.VMEM((3, tall, groups, part, wide), bf16),
            pltpu.VMEM((groups, broad, tall * tall_slab, columns), bf16),
            pltpu.VMEM((3, tall, block, wide), bf16),
            pltpu.VMEM((3, length, wide), bf16),
            pltpu.VMEM((heads, tall, block, 2 * width), bf16),
            pltpu.VMEM((heads, tall, width + 16, block), bf16),
            pltpu.VMEM((tall, heads, block), jnp.float32),
            pltpu.VMEM((tall, broad, span, rows), bf16),
            pltpu.VMEM((count, span, rows), bf16),
            pltpu.VMEM((tall, broad, rows, wide), bf16),
            pltpu.VMEM((count, rows, wide), bf16),
            pltpu.VMEM((tall, broad, 8, rows), jnp.float32),
            pltpu.VMEM((count, 8, rows), jnp.float32),
            sem((others,)), sem((others,)),
            sem((3, tall, 2)), sem((3, tall, beside)), sem((3, tall, across)),
            sem((3, tall, groups)),
            sem((3, broad, tall)), sem((3, count)),
            sem((tall, 2)), sem((tall,)), sem((others,)), sem((broad,)),
            sem((broad, beside)), sem((across, broad)), sem((across, broad)), sem((across, broad)),
            sem((tall, broad)), sem((count,)),
            sem((tall, broad)), sem((count,)), sem((tall,)), sem((tall,)),
            sem((tall, broad)), sem((count,)),
        ],
        compiler_params=pltpu.CompilerParams(
            collective_id=0, has_side_effects=True, vmem_limit_bytes=60 * 1024 * 1024
        ),
    )(own_rows, w_query, w_key, w_value, w_output, qk_gain, decay_rows)
    return result[None]


def solution(mesh):
    placed = (
        P("dp", "sp", None),
        P("dp", "sp"),
        P("dp", "sp"),
        P("dp", "sp"),
        P("sp", "dp"),
        P(),
        P("dp", "sp", None),
    )
    return jax.shard_map(
        on_device, mesh=mesh, in_specs=placed, out_specs=P("dp", "sp", None), check_vma=False
    )
```

```python
import functools

import jax
import jax.numpy as jnp
from jax import lax
from jax.experimental import pallas as pl
from jax.experimental.pallas import tpu as pltpu
from jax.sharding import PartitionSpec as P

EPS = 1e-06
DIMS_NT = (((1,), (1,)), ((), ()))
MESH = pl.DeviceIdType.MESH
CORES = 2


def layout(count, groups):
    tall = 4 if count % 4 == 0 else 1
    return tall, count // tall, groups // CORES


def layer_kernel(
    heads, width, count, groups,
    own_ref, wq_ref, wk_ref, wv_ref, slab_ref, gain_ref, decay_ref, out_ref,
    far_ref, weight_ref, slabs_ref, stage_ref, full_ref, key_ref, value_ref, home_decay_ref,
    near_stage_ref, near_ref, done_ref, merged_ref, log_ref, logs_ref,
    far_send, far_recv, wz_send, wx_send, wc_send, w_recv, move_send, move_recv,
    sz_send, sz_recv, sy_send, sy_recv, sx_send, sx_recv, sc_send, sc_recv, done_send, done_recv,
    near_send, near_recv, decay_send, decay_recv, log_send, log_recv,
):
    rows, depth = own_ref.shape
    part = wq_ref.shape[0]
    wide = heads * width
    tall, broad, across = layout(count, groups)
    block = broad * rows
    span = wide + 16
    me, group = lax.axis_index("sp"), lax.axis_index("dp")
    z, y = me // broad, lax.rem(me, broad)
    x, core = group // CORES, lax.rem(group, CORES)
    partner = x * CORES + 1 - core

    def plane(shift):
        return lax.rem(z + shift, tall)

    def along_x(shift):
        return lax.rem(x + shift, across)

    def along_y(shift):
        return lax.rem(y + shift, broad)

    barrier = pltpu.get_barrier_semaphore()
    for shift in range(1, count):
        other = lax.rem(me + shift, count)
        pl.semaphore_signal(barrier, inc=1, device_id={"sp": other}, device_id_type=MESH)
    for shift in range(1, groups):
        peer = lax.rem(group + shift, groups)
        pl.semaphore_signal(barrier, inc=1, device_id={"dp": peer}, device_id_type=MESH)
    pl.semaphore_wait(barrier, count + groups - 2)

    def remote(source, target, out_sem, in_sem, device):
        return pltpu.make_async_remote_copy(
            src_ref=source, dst_ref=target, send_sem=out_sem, recv_sem=in_sem,
            device_id=device, device_id_type=MESH,
        )

    tokens = [
        remote(
            own_ref, far_ref.at[broad - shift - 1], far_send.at[shift - 1],
            far_recv.at[broad - shift - 1], {"sp": z * broad + along_y(shift)},
        )
        for shift in range(1, broad)
    ]

    chunks = (wk_ref, wv_ref, wq_ref)
    weights = [weight_ref.at[number] for number in range(3)]

    def weight(number, level, owner, out_sem, device):
        piece = weights[number].at[level, owner]
        return remote(piece, piece, out_sem, w_recv.at[number, level, owner], device)

    def up(number, level):
        return weight(
            number, level, group, wz_send.at[number, level, 0], {"sp": (z + 1) * broad + y}
        )

    def down(number, level):
        return weight(
            number, level, group, wz_send.at[number, level, 1], {"sp": (z - 1) * broad + y}
        )

    def sideways(number, level):
        return [
            weight(
                number, level, group, wx_send.at[number, level, shift - 1],
                {"dp": along_x(shift) * CORES + core},
            )
            for shift in range(1, across)
        ]

    def to_core(number, level, column):
        return weight(
            number, level, column * CORES + core, wc_send.at[number, level, column],
            {"dp": partner},
        )

    def own_along_z(number):
        @pl.when(z + 1 < tall)
        def _():
            up(number, z).start()

        @pl.when(z > 0)
        def _():
            down(number, z).start()

    def spread(number, level):
        for copy in sideways(number, level):
            copy.start()
        to_core(number, level, x).start()

    def relay(number, distance, onward=True, across_too=True):
        for way, step in enumerate((up, down)):
            level = z - distance if way == 0 else z + distance
            inside = (level >= 0) if way == 0 else (level < tall)
            more = (z + 1 < tall) if way == 0 else (z > 0)

            @pl.when(inside)
            def _():
                if onward:
                    step(number, level).wait_recv()

                    @pl.when(more)
                    def _():
                        step(number, level).start()

                if across_too:
                    spread(number, level)

    def relay_core(number):
        for turn in range(tall):
            for shift in range(1, across):
                level, column = plane(turn), along_x(shift)
                copy = to_core(number, level, column)
                weight(
                    number, level, column * CORES + core, wc_send.at[number, level, column],
                    {"dp": partner},
                ).wait_recv()
                copy.start()

    def gathered(number):
        for turn in range(tall):
            for column in range(across):
                level = plane(turn)
                weight(
                    number, level, column * CORES + 1 - core, wc_send.at[number, level, column],
                    {"dp": partner},
                ).wait_recv()

    def weights_sent(number):
        for turn in range(tall):
            level = plane(turn)

            @pl.when((level <= z) & (z + 1 < tall))
            def _():
                up(number, level).wait_send()

            @pl.when((level >= z) & (z > 0))
            def _():
                down(number, level).wait_send()

            for copy in sideways(number, level):
                copy.wait_send()
            for column in range(across):
                to_core(number, level, column).wait_send()

    def home_decay(turn):
        place = pl.ds(pl.multiple_of(plane(turn) * block, block), block)
        return remote(
            decay_ref.at[:, place], home_decay_ref.at[z], decay_send.at[turn], decay_recv.at[z],
            {"sp": plane(turn) * broad + y},
        )

    lane = lax.broadcasted_iota(jnp.int32, (rows, wide), 1)

    def unit(values, gain):
        values = values.astype(jnp.bfloat16).astype(jnp.float32)
        squares = values * values
        scale = jnp.zeros_like(values)
        for head in range(heads):
            inside = (lane >= head * width) & (lane < (head + 1) * width)
            total = jnp.sum(jnp.where(inside, squares, 0.0), axis=-1, keepdims=True)
            scale = jnp.where(inside, lax.rsqrt(total / width + EPS), scale)
        gains = jnp.concatenate([gain] * heads, axis=1)
        return values * scale * gains

    def row_place(source):
        return pl.ds(pl.multiple_of(source * rows, rows), rows)

    def move(number, turn, side):
        column = along_y(side)
        source = z * broad + column
        return remote(
            stage_ref.at[number, turn, row_place(column)],
            full_ref.at[number, row_place(source)],
            move_send.at[number, side, turn], move_recv.at[number, source],
            {"sp": plane(turn) * broad + y},
        )

    def needed(number, level):
        return (level > 0) if number == 2 else (level < tall - 1)

    turns = sorted(range(tall), key=lambda turn: (turn == 0, turn != tall // 2))

    def project(number, side):
        values = own_ref[...] if side == 0 else far_ref[side - 1]
        bunch = 2 if wide % 128 == 0 and tall % 2 == 0 else 1
        for first in range(0, tall, bunch):
            some = turns[first : first + bunch]
            columns = [weights[number][plane(turn)].reshape(depth, wide) for turn in some]
            result = jnp.dot(
                values, columns[0] if bunch == 1 else jnp.concatenate(columns, axis=1),
                preferred_element_type=jnp.float32,
            )
            for index, turn in enumerate(some):
                piece = result[:, index * wide : (index + 1) * wide]
                if number == 0:
                    piece = unit(piece, gain_ref[1:2, :])
                elif number == 2:
                    piece = unit(piece, gain_ref[0:1, :]) * width ** (-0.5)
                piece = piece.astype(jnp.bfloat16)
                stage_ref[number, turn, row_place(along_y(side)), :] = piece
                if turn == 0:
                    full_ref[number, row_place(z * broad + along_y(side)), :] = piece
            for turn in some:
                if turn:
                    @pl.when(needed(number, z))
                    def _():
                        move(number, turn, side).start()

    def moved(number, level):
        @pl.when((level != z) & needed(number, level))
        def _():
            for column in range(broad):
                source = level * broad + column
                target = full_ref.at[number, row_place(source)]
                remote(
                    target, target, move_send.at[number, 0, 0], move_recv.at[number, source],
                    {"sp": source},
                ).wait_recv()

    tall_slab = slab_ref.shape[0]

    def slab_z(level, way):
        place = pl.ds(pl.multiple_of(level * tall_slab, tall_slab), tall_slab)
        piece = slabs_ref.at[group, y, place]
        return remote(
            piece, piece, sz_send.at[level, way], sz_recv.at[level],
            {"sp": (z + 1 - 2 * way) * broad + y},
        )

    def slab_relay(distance):
        for way in range(2):
            level = z - distance if way == 0 else z + distance
            inside = (level >= 0) if way == 0 else (level < tall)
            onward = (z + 1 < tall) if way == 0 else (z > 0)
            if distance:
                @pl.when(inside)
                def _():
                    slab_z(level, way).wait_recv()

            @pl.when(inside & onward)
            def _():
                slab_z(level, way).start()

    def slab_y(shift):
        piece = slabs_ref.at[group, y]
        return remote(
            piece, piece, sy_send.at[shift - 1], sy_recv.at[y],
            {"sp": z * broad + along_y(shift)},
        )

    def slab_x(column, shift):
        piece = slabs_ref.at[group, column]
        return remote(
            piece, piece, sx_send.at[column, shift - 1], sx_recv.at[x, column],
            {"dp": along_x(shift) * CORES + core},
        )

    def slab_core(level, column):
        piece = slabs_ref.at[level * CORES + core, column]
        return remote(
            piece, piece, sc_send.at[level, column], sc_recv.at[level, column], {"dp": partner}
        )

    def slab_spread(column):
        for shift in range(1, across):
            slab_x(column, shift).start()
        slab_core(x, column).start()

    def slabs_of_z_along_y():
        for shift in range(1, broad):
            slab_y(shift).start()

    def slabs_from_y():
        for shift in range(1, broad):
            column = along_y(shift)
            piece = slabs_ref.at[group, column]
            remote(
                piece, piece, sy_send.at[shift - 1], sy_recv.at[column], {"sp": me}
            ).wait_recv()
            slab_spread(column)

    def slabs_from_x():
        for turn in range(broad):
            column = along_y(turn)
            for shift in range(1, across):
                level = along_x(shift)
                piece = slabs_ref.at[level * CORES + core, column]
                remote(
                    piece, piece, sx_send.at[column, shift - 1], sx_recv.at[level, column],
                    {"dp": group},
                ).wait_recv()
                slab_core(level, column).start()

    def slabs_from_core():
        for level in range(across):
            for column in range(broad):
                piece = slabs_ref.at[level * CORES + 1 - core, column]
                remote(
                    piece, piece, sc_send.at[level, column], sc_recv.at[level, column],
                    {"dp": partner},
                ).wait_recv()

    for number in range(3):
        weight_ref[number, z, group] = chunks[number][...]
        if number < 2:
            own_along_z(number)
            spread(number, z)
        if number == 0:
            for copy in tokens:
                copy.start()
            slabs_ref[
                group, y, pl.ds(pl.multiple_of(z * tall_slab, tall_slab), tall_slab), :
            ] = slab_ref[...]
    for turn in range(1, tall):
        home_decay(turn).start()
    home_decay_ref[z] = decay_ref[:, pl.ds(pl.multiple_of(z * block, block), block)]

    def ready(number):
        relay_core(number)
        gathered(number)

    def steps(*distances):
        return [distance for distance in distances if distance < tall]

    for distance in range(1, tall):
        relay(0, distance)
        if distance == 1:
            relay(1, 1, across_too=False)
            own_along_z(2)
            slab_relay(0)
        elif distance == 2:
            relay(1, 1, onward=False)
            relay(1, 2, across_too=False)
    if tall > 1:
        relay(2, 1, across_too=False)
    if tall > 2:
        relay(1, 2, onward=False)
    if tall > 1:
        slab_relay(1)
    ready(0)
    for distance in range(3, tall):
        relay(1, distance)
    project(0, 0)
    spread(2, z)
    if tall > 1:
        relay(2, 1, onward=False)
    if tall > 2:
        relay(2, 2)
        slab_relay(2)
    ready(1)
    for distance in range(3, tall):
        relay(2, distance)
    project(1, 0)
    for copy in tokens:
        copy.wait_recv()
    for number in range(2):
        for side in range(1, broad):
            project(number, side)
    for distance in range(3, tall):
        slab_relay(distance)
    slabs_of_z_along_y()
    slab_spread(y)
    ready(2)
    for side in range(broad):
        project(2, side)

    def split(values):
        first = values.astype(jnp.bfloat16).astype(jnp.float32)
        rest = values - first
        second = rest.astype(jnp.bfloat16).astype(jnp.float32)
        return first, second, rest - second

    block_lane = lax.broadcasted_iota(jnp.int32, (block, 2 * width), 1)
    ones_rows = jnp.where(lax.broadcasted_iota(jnp.int32, (16, block), 0) == 0, 1.0, 0.0)
    packed = wide == 2 * width

    def aside(head):
        return width if packed and head == 0 else 0

    def beside(head):
        low = aside(head)
        return (block_lane >= low) & (block_lane < low + width)

    def with_lanes(values, head, lanes):
        if packed:
            return jnp.where(beside(head), lanes, values.astype(jnp.float32)).astype(jnp.bfloat16)
        own = values[:, head * width : (head + 1) * width].astype(jnp.float32)
        return jnp.concatenate([lanes[:, :width], own], axis=1).astype(jnp.bfloat16)

    def query_operand(values, head):
        low = aside(head)
        ones = jnp.where((block_lane >= low) & (block_lane < low + 3), 1.0, 0.0)
        return with_lanes(values, head, ones)

    def key_operands(values, decay):
        sub = lax.broadcasted_iota(jnp.int32, (2 * width, block), 0)
        lanes = jnp.zeros((2 * width, block), jnp.float32)
        fresh = []
        for head in range(heads):
            for index, piece in enumerate(split(-decay[head : head + 1, :])):
                lanes = jnp.where(sub == aside(head) + index, piece, lanes)
            if not packed:
                fresh.append(with_lanes(values, head, lanes.T))
        if packed:
            turned = lanes.T
            fresh = [with_lanes(values, head, turned) for head in range(heads)]
        return fresh

    def value_operands(values):
        turned = values.astype(jnp.float32).T
        return [
            jnp.concatenate(
                [turned[head * width : (head + 1) * width], ones_rows], axis=0
            ).astype(jnp.bfloat16)
            for head in range(heads)
        ]

    def averages(parts):
        mixed, logs = [], []
        for peak, total in parts:
            norm = total[width : width + 1]
            mixed.append(total[:width] / norm)
            logs.append(peak + jnp.log(norm))
        return mixed, logs

    def pieces(values):
        return [
            (pltpu.roll(values, block - column * rows, 1) if column else values)[:, :rows]
            for column in range(broad)
        ]

    def stacked(rows_of, extent):
        sub = lax.broadcasted_iota(jnp.int32, (extent, block), 0)
        result = jnp.zeros((extent, block), jnp.float32)
        for index, piece in enumerate(rows_of):
            result = jnp.where(sub == index, piece, result)
        return result

    def scores_of(keys, queries):
        return lax.dot_general(keys, queries, DIMS_NT, preferred_element_type=jnp.float32)

    def online(carry, keys, queries, values):
        peak, total = carry
        scores = scores_of(keys, queries)
        higher = jnp.maximum(peak, jnp.max(scores, axis=0, keepdims=True))
        probs = jnp.exp(scores - higher).astype(jnp.bfloat16)
        total = total * jnp.exp(peak - higher) + jnp.dot(
            values, probs, preferred_element_type=jnp.float32
        )
        return higher, total

    def near_copy(turn, side):
        column = along_y(side)
        return remote(
            near_stage_ref.at[turn, column], near_ref.at[plane(turn) * broad + y],
            near_send.at[turn, side], near_recv.at[plane(turn) * broad + y],
            {"sp": z * broad + column},
        )

    key_place = lax.broadcasted_iota(jnp.int32, (block, block), 0)
    query_place = lax.broadcasted_iota(jnp.int32, (block, block), 1)

    def near_block(turn, unused):
        keys = key_operands(stage_ref[0, turn], home_decay_ref[plane(turn)])
        values = value_operands(stage_ref[1, turn])
        parts = []
        for head in range(heads):
            scores = scores_of(keys[head], query_operand(stage_ref[2, turn], head))
            scores = jnp.where(key_place <= query_place, scores, -jnp.inf)
            peak = jnp.max(scores, axis=0, keepdims=True)
            probs = jnp.exp(scores - peak).astype(jnp.bfloat16)
            parts.append(
                (peak, jnp.dot(values[head], probs, preferred_element_type=jnp.float32))
            )
        mixed, logs = averages(parts)
        tail = stacked([piece for log in logs for piece in split(log)], 16)
        for column, piece in enumerate(pieces(jnp.concatenate([*mixed, tail], axis=0))):
            near_stage_ref[turn, column] = piece.astype(jnp.bfloat16)
        near_ref[plane(turn) * broad + y] = near_stage_ref[turn, y]
        for side in range(1, broad):
            near_copy(turn, side).start()

        return unused

    for turn in range(1, tall):
        remote(
            home_decay_ref.at[plane(turn)], home_decay_ref.at[plane(turn)], decay_send.at[turn],
            decay_recv.at[plane(turn)], {"sp": me},
        ).wait_recv()
    slabs_from_y()
    lax.fori_loop(0, tall, near_block, 0)

    def prepare(level):
        moved(0, level)
        moved(1, level)
        place = pl.ds(pl.multiple_of(level * block, block), block)
        keys = key_operands(full_ref[0, place, :], decay_ref[:, place])
        values = value_operands(full_ref[1, place, :])
        for head in range(heads):
            key_ref[head, level] = keys[head]
            value_ref[head, level] = values[head]

    def remote_done(level, column):
        device = {"sp": level * broad + column}
        return [
            remote(
                done_ref.at[level, column], merged_ref.at[me], done_send.at[level, column],
                done_recv.at[me], device,
            ),
            remote(
                log_ref.at[level, column], logs_ref.at[me], log_send.at[level, column],
                log_recv.at[me], device,
            ),
        ]

    def far_block(index, unused):
        level = lax.rem(index + 1, max(tall - 1, 1)) + 1
        for column in range(tall - 1):
            @pl.when(index == max(column - 1, 0))
            def _():
                prepare(column)

        moved(2, level)
        place = pl.ds(pl.multiple_of(level * block, block), block)
        queries = [query_operand(full_ref[2, place, :], head) for head in range(heads)]

        def step(column, carry):
            return tuple(
                online(carry[head], key_ref[head, column], queries[head], value_ref[head, column])
                for head in range(heads)
            )

        start = tuple(
            (
                jnp.full((1, block), -1e30, jnp.float32),
                jnp.zeros((width + 16, block), jnp.float32),
            )
            for _ in range(heads)
        )
        carry = lax.fori_loop(0, level, step, start)
        mixed, logs = averages(carry)
        turned = jnp.concatenate(mixed, axis=0).T.astype(jnp.bfloat16)
        for column, piece in enumerate(pieces(stacked(logs, 8))):
            log_ref[level, column] = piece
            done_ref[level, column] = turned[column * rows : (column + 1) * rows]

            @pl.when(level * broad + column != me)
            def _():
                for copy in remote_done(level, column):
                    copy.start()

        @pl.when(index == min(1, tall - 2))
        def _():
            slabs_from_x()

        return unused

    lax.fori_loop(0, tall - 1, far_block, 0)

    @pl.when(z > 0)
    def _():
        merged_ref[me] = done_ref[z, y]
        logs_ref[me] = log_ref[z, y]
        for shift in range(1, count):
            source = lax.rem(me + shift, count)
            remote(
                merged_ref.at[source], merged_ref.at[source], done_send.at[0, 0],
                done_recv.at[source], {"sp": source},
            ).wait_recv()
            remote(
                logs_ref.at[source], logs_ref.at[source], log_send.at[0, 0],
                log_recv.at[source], {"sp": source},
            ).wait_recv()

    @pl.when(z == 0)
    def _():
        for source in range(count):
            merged_ref[source] = jnp.zeros((rows, wide), jnp.bfloat16)
            logs_ref[source] = jnp.full((8, rows), -1e30, jnp.float32)

    for turn in range(tall):
        for side in range(1, broad):
            target = near_ref.at[plane(turn) * broad + along_y(side)]
            remote(
                target, target, near_send.at[turn, side],
                near_recv.at[plane(turn) * broad + along_y(side)], {"sp": me},
            ).wait_recv()
    slabs_from_core()

    def combined(source):
        one = near_ref[source].astype(jnp.float32)
        two = merged_ref[source].astype(jnp.float32).T
        outs = []
        for head in range(heads):
            low = wide + 3 * head
            near_log = sum(one[low + i : low + i + 1] for i in range(3))
            logs = near_log, logs_ref[source][head : head + 1]
            peak = jnp.maximum(*logs)
            first, second = (jnp.exp(log - peak) for log in logs)
            norm = first + second
            place = slice(head * width, (head + 1) * width)
            mixed = one[place] * (first / norm) + two[place] * (second / norm)
            scale = lax.rsqrt(jnp.mean(mixed * mixed, axis=0, keepdims=True) + EPS)
            outs.append(mixed * scale)
        return jnp.concatenate(outs, axis=0).T.astype(jnp.bfloat16)

    merged = jnp.concatenate(
        [combined(level * broad + column) for column in range(broad) for level in range(tall)],
        axis=1,
    )
    columns = slab_ref.shape[1]
    for place in range(groups):
        out_ref[:, place * columns : (place + 1) * columns] = jnp.dot(
            merged, slabs_ref[place].reshape(-1, columns), preferred_element_type=jnp.float32
        ).astype(out_ref.dtype)

    for copy in tokens:
        copy.wait_send()
    for number in range(3):
        weights_sent(number)

        @pl.when(needed(number, z))
        def _():
            for side in range(broad):
                for turn in range(1, tall):
                    move(number, turn, side).wait_send()
    for turn in range(tall):
        if turn:
            home_decay(turn).wait_send()
        for side in range(1, broad):
            near_copy(turn, side).wait_send()
    for distance in range(tall):
        for way in range(2):
            level = z - distance if way == 0 else z + distance
            inside = (level >= 0) if way == 0 else (level < tall)
            onward = (z + 1 < tall) if way == 0 else (z > 0)

            @pl.when(inside & onward)
            def _():
                slab_z(level, way).wait_send()

    for shift in range(1, broad):
        slab_y(shift).wait_send()
    for column in range(broad):
        for shift in range(1, across):
            slab_x(column, shift).wait_send()
        for level in range(across):
            slab_core(level, column).wait_send()
    for level in range(1, tall):
        for column in range(broad):
            @pl.when(level * broad + column != me)
            def _():
                for copy in remote_done(level, column):
                    copy.wait_send()


def on_device(tokens, w_query, w_key, w_value, w_output, qk_gain, decay_sums):
    own_rows, decay_rows = tokens[0], decay_sums[0]
    count, groups = lax.axis_size("sp"), lax.axis_size("dp")
    tall, broad, across = layout(count, groups)
    rows, depth = own_rows.shape
    part = w_query.shape[0]
    heads, width = decay_rows.shape[0], qk_gain.shape[1]
    wide, length, block = heads * width, count * rows, broad * rows
    tall_slab, columns = w_output.shape
    bf16, sem, span = jnp.bfloat16, pltpu.SemaphoreType.DMA, wide + 16
    others, beside = max(broad - 1, 1), max(across - 1, 1)
    result = pl.pallas_call(
        functools.partial(layer_kernel, heads, width, count, groups),
        out_shape=jax.ShapeDtypeStruct((rows, depth), bf16),
        in_specs=[pl.BlockSpec(memory_space=pltpu.VMEM)] * 7,
        out_specs=pl.BlockSpec(memory_space=pltpu.VMEM),
        scratch_shapes=[
            pltpu.VMEM((others, rows, depth), bf16),
            pltpu.VMEM((3, tall, groups, part, wide), bf16),
            pltpu.VMEM((groups, broad, tall * tall_slab, columns), bf16),
            pltpu.VMEM((3, tall, block, wide), bf16),
            pltpu.VMEM((3, length, wide), bf16),
            pltpu.VMEM((heads, tall, block, 2 * width), bf16),
            pltpu.VMEM((heads, tall, width + 16, block), bf16),
            pltpu.VMEM((tall, heads, block), jnp.float32),
            pltpu.VMEM((tall, broad, span, rows), bf16),
            pltpu.VMEM((count, span, rows), bf16),
            pltpu.VMEM((tall, broad, rows, wide), bf16),
            pltpu.VMEM((count, rows, wide), bf16),
            pltpu.VMEM((tall, broad, 8, rows), jnp.float32),
            pltpu.VMEM((count, 8, rows), jnp.float32),
            sem((others,)), sem((others,)),
            sem((3, tall, 2)), sem((3, tall, beside)), sem((3, tall, across)),
            sem((3, tall, groups)),
            sem((3, broad, tall)), sem((3, count)),
            sem((tall, 2)), sem((tall,)), sem((others,)), sem((broad,)),
            sem((broad, beside)), sem((across, broad)), sem((across, broad)), sem((across, broad)),
            sem((tall, broad)), sem((count,)),
            sem((tall, broad)), sem((count,)), sem((tall,)), sem((tall,)),
            sem((tall, broad)), sem((count,)),
        ],
        compiler_params=pltpu.CompilerParams(
            collective_id=0, has_side_effects=True, vmem_limit_bytes=60 * 1024 * 1024
        ),
    )(own_rows, w_query, w_key, w_value, w_output, qk_gain, decay_rows)
    return result[None]


def solution(mesh):
    placed = (
        P("dp", "sp", None),
        P("dp", "sp"),
        P("dp", "sp"),
        P("dp", "sp"),
        P("sp", "dp"),
        P(),
        P("dp", "sp", None),
    )
    return jax.shard_map(
        on_device, mesh=mesh, in_specs=placed, out_specs=P("dp", "sp", None), check_vma=False
    )
```

```python
import functools

import jax
import jax.numpy as jnp
from jax import lax
from jax.experimental import pallas as pl
from jax.experimental.pallas import tpu as pltpu
from jax.sharding import PartitionSpec as P

EPS = 1e-06
DIMS_NT = (((1,), (1,)), ((), ()))
MESH = pl.DeviceIdType.MESH
CORES = 2


def layout(count, groups):
    tall = 4 if count % 4 == 0 else 1
    return tall, count // tall, groups // CORES


def layer_kernel(
    heads, width, count, groups,
    own_ref, wq_ref, wk_ref, wv_ref, slab_ref, gain_ref, decay_ref, out_ref,
    far_ref, weight_ref, slabs_ref, stage_ref, full_ref, key_ref, value_ref, home_decay_ref,
    near_stage_ref, near_ref, done_ref, merged_ref, log_ref, logs_ref,
    far_send, far_recv, wz_send, wx_send, wc_send, w_recv, move_send, move_recv,
    sz_send, sz_recv, sy_send, sy_recv, sx_send, sx_recv, sc_send, sc_recv, done_send, done_recv,
    near_send, near_recv, decay_send, decay_recv, log_send, log_recv,
):
    rows, depth = own_ref.shape
    part = wq_ref.shape[0]
    wide = heads * width
    tall, broad, across = layout(count, groups)
    block = broad * rows
    span = wide + 16
    me, group = lax.axis_index("sp"), lax.axis_index("dp")
    z, y = me // broad, lax.rem(me, broad)
    x, core = group // CORES, lax.rem(group, CORES)
    partner = x * CORES + 1 - core

    def plane(shift):
        return lax.rem(z + shift, tall)

    def along_x(shift):
        return lax.rem(x + shift, across)

    def along_y(shift):
        return lax.rem(y + shift, broad)

    barrier = pltpu.get_barrier_semaphore()
    for shift in range(1, count):
        other = lax.rem(me + shift, count)
        pl.semaphore_signal(barrier, inc=1, device_id={"sp": other}, device_id_type=MESH)
    for shift in range(1, groups):
        peer = lax.rem(group + shift, groups)
        pl.semaphore_signal(barrier, inc=1, device_id={"dp": peer}, device_id_type=MESH)
    pl.semaphore_wait(barrier, count + groups - 2)

    def remote(source, target, out_sem, in_sem, device):
        return pltpu.make_async_remote_copy(
            src_ref=source, dst_ref=target, send_sem=out_sem, recv_sem=in_sem,
            device_id=device, device_id_type=MESH,
        )

    tokens = [
        remote(
            own_ref, far_ref.at[broad - shift - 1], far_send.at[shift - 1],
            far_recv.at[broad - shift - 1], {"sp": z * broad + along_y(shift)},
        )
        for shift in range(1, broad)
    ]

    chunks = (wk_ref, wv_ref, wq_ref)
    weights = [weight_ref.at[number] for number in range(3)]

    def weight(number, level, owner, out_sem, device):
        piece = weights[number].at[level, owner]
        return remote(piece, piece, out_sem, w_recv.at[number, level, owner], device)

    def up(number, level):
        return weight(
            number, level, group, wz_send.at[number, level, 0], {"sp": (z + 1) * broad + y}
        )

    def down(number, level):
        return weight(
            number, level, group, wz_send.at[number, level, 1], {"sp": (z - 1) * broad + y}
        )

    def sideways(number, level):
        return [
            weight(
                number, level, group, wx_send.at[number, level, shift - 1],
                {"dp": along_x(shift) * CORES + core},
            )
            for shift in range(1, across)
        ]

    def to_core(number, level, column):
        return weight(
            number, level, column * CORES + core, wc_send.at[number, level, column],
            {"dp": partner},
        )

    def own_along_z(number):
        @pl.when(z + 1 < tall)
        def _():
            up(number, z).start()

        @pl.when(z > 0)
        def _():
            down(number, z).start()

    def spread(number, level):
        for copy in sideways(number, level):
            copy.start()
        to_core(number, level, x).start()

    def relay(number, distance, onward=True, across_too=True):
        for way, step in enumerate((up, down)):
            level = z - distance if way == 0 else z + distance
            inside = (level >= 0) if way == 0 else (level < tall)
            more = (z + 1 < tall) if way == 0 else (z > 0)

            @pl.when(inside)
            def _():
                if onward:
                    step(number, level).wait_recv()

                    @pl.when(more)
                    def _():
                        step(number, level).start()

                if across_too:
                    spread(number, level)

    def relay_core(number):
        for turn in range(tall):
            for shift in range(1, across):
                level, column = plane(turn), along_x(shift)
                copy = to_core(number, level, column)
                weight(
                    number, level, column * CORES + core, wc_send.at[number, level, column],
                    {"dp": partner},
                ).wait_recv()
                copy.start()

    def gathered(number):
        for turn in range(tall):
            for column in range(across):
                level = plane(turn)
                weight(
                    number, level, column * CORES + 1 - core, wc_send.at[number, level, column],
                    {"dp": partner},
                ).wait_recv()

    def weights_sent(number):
        for turn in range(tall):
            level = plane(turn)

            @pl.when((level <= z) & (z + 1 < tall))
            def _():
                up(number, level).wait_send()

            @pl.when((level >= z) & (z > 0))
            def _():
                down(number, level).wait_send()

            for copy in sideways(number, level):
                copy.wait_send()
            for column in range(across):
                to_core(number, level, column).wait_send()

    def home_decay(turn):
        place = pl.ds(pl.multiple_of(plane(turn) * block, block), block)
        return remote(
            decay_ref.at[:, place], home_decay_ref.at[z], decay_send.at[turn], decay_recv.at[z],
            {"sp": plane(turn) * broad + y},
        )

    lane = lax.broadcasted_iota(jnp.int32, (rows, wide), 1)

    def unit(values, gain):
        values = values.astype(jnp.bfloat16).astype(jnp.float32)
        squares = values * values
        scale = jnp.zeros_like(values)
        for head in range(heads):
            inside = (lane >= head * width) & (lane < (head + 1) * width)
            total = jnp.sum(jnp.where(inside, squares, 0.0), axis=-1, keepdims=True)
            scale = jnp.where(inside, lax.rsqrt(total / width + EPS), scale)
        gains = jnp.concatenate([gain] * heads, axis=1)
        return values * scale * gains

    def row_place(source):
        return pl.ds(pl.multiple_of(source * rows, rows), rows)

    def move(number, turn, side):
        column = along_y(side)
        source = z * broad + column
        return remote(
            stage_ref.at[number, turn, row_place(column)],
            full_ref.at[number, row_place(source)],
            move_send.at[number, side, turn], move_recv.at[number, source],
            {"sp": plane(turn) * broad + y},
        )

    def needed(number, level):
        return (level > 0) if number == 2 else (level < tall - 1)

    turns = sorted(range(tall), key=lambda turn: (turn == 0, turn != tall // 2))

    def project(number, side):
        values = own_ref[...] if side == 0 else far_ref[side - 1]
        bunch = 2 if wide % 128 == 0 and tall % 2 == 0 else 1
        for first in range(0, tall, bunch):
            some = turns[first : first + bunch]
            columns = [weights[number][plane(turn)].reshape(depth, wide) for turn in some]
            result = jnp.dot(
                values, columns[0] if bunch == 1 else jnp.concatenate(columns, axis=1),
                preferred_element_type=jnp.float32,
            )
            for index, turn in enumerate(some):
                piece = result[:, index * wide : (index + 1) * wide]
                if number == 0:
                    piece = unit(piece, gain_ref[1:2, :])
                elif number == 2:
                    piece = unit(piece, gain_ref[0:1, :]) * width ** (-0.5)
                piece = piece.astype(jnp.bfloat16)
                stage_ref[number, turn, row_place(along_y(side)), :] = piece
                if turn == 0:
                    full_ref[number, row_place(z * broad + along_y(side)), :] = piece
            for turn in some:
                if turn:
                    @pl.when(needed(number, z))
                    def _():
                        move(number, turn, side).start()

    def moved(number, level):
        @pl.when((level != z) & needed(number, level))
        def _():
            for column in range(broad):
                source = level * broad + column
                target = full_ref.at[number, row_place(source)]
                remote(
                    target, target, move_send.at[number, 0, 0], move_recv.at[number, source],
                    {"sp": source},
                ).wait_recv()

    tall_slab = slab_ref.shape[0]

    def slab_z(level, way):
        place = pl.ds(pl.multiple_of(level * tall_slab, tall_slab), tall_slab)
        piece = slabs_ref.at[group, y, place]
        return remote(
            piece, piece, sz_send.at[level, way], sz_recv.at[level],
            {"sp": (z + 1 - 2 * way) * broad + y},
        )

    def slab_relay(distance):
        for way in range(2):
            level = z - distance if way == 0 else z + distance
            inside = (level >= 0) if way == 0 else (level < tall)
            onward = (z + 1 < tall) if way == 0 else (z > 0)
            if distance:
                @pl.when(inside)
                def _():
                    slab_z(level, way).wait_recv()

            @pl.when(inside & onward)
            def _():
                slab_z(level, way).start()

    def slab_y(shift):
        piece = slabs_ref.at[group, y]
        return remote(
            piece, piece, sy_send.at[shift - 1], sy_recv.at[y],
            {"sp": z * broad + along_y(shift)},
        )

    def slab_x(column, shift):
        piece = slabs_ref.at[group, column]
        return remote(
            piece, piece, sx_send.at[column, shift - 1], sx_recv.at[x, column],
            {"dp": along_x(shift) * CORES + core},
        )

    def slab_core(level, column):
        piece = slabs_ref.at[level * CORES + core, column]
        return remote(
            piece, piece, sc_send.at[level, column], sc_recv.at[level, column], {"dp": partner}
        )

    def slab_spread(column):
        for shift in range(1, across):
            slab_x(column, shift).start()
        slab_core(x, column).start()

    def slabs_of_z_along_y():
        for shift in range(1, broad):
            slab_y(shift).start()

    def slabs_from_y():
        for shift in range(1, broad):
            column = along_y(shift)
            piece = slabs_ref.at[group, column]
            remote(
                piece, piece, sy_send.at[shift - 1], sy_recv.at[column], {"sp": me}
            ).wait_recv()
            slab_spread(column)

    def slabs_from_x():
        for turn in range(broad):
            column = along_y(turn)
            for shift in range(1, across):
                level = along_x(shift)
                piece = slabs_ref.at[level * CORES + core, column]
                remote(
                    piece, piece, sx_send.at[column, shift - 1], sx_recv.at[level, column],
                    {"dp": group},
                ).wait_recv()
                slab_core(level, column).start()

    def slabs_from_core():
        for level in range(across):
            for column in range(broad):
                piece = slabs_ref.at[level * CORES + 1 - core, column]
                remote(
                    piece, piece, sc_send.at[level, column], sc_recv.at[level, column],
                    {"dp": partner},
                ).wait_recv()

    for number in range(3):
        weight_ref[number, z, group] = chunks[number][...]
        if number < 2:
            own_along_z(number)
            spread(number, z)
        if number == 0:
            for copy in tokens:
                copy.start()
            slabs_ref[
                group, y, pl.ds(pl.multiple_of(z * tall_slab, tall_slab), tall_slab), :
            ] = slab_ref[...]
    for turn in range(1, tall):
        home_decay(turn).start()
    home_decay_ref[z] = decay_ref[:, pl.ds(pl.multiple_of(z * block, block), block)]

    def ready(number):
        relay_core(number)
        gathered(number)

    def steps(*distances):
        return [distance for distance in distances if distance < tall]

    for distance in range(1, tall):
        relay(0, distance)
        if distance == 1:
            relay(1, 1, across_too=False)
            own_along_z(2)
            slab_relay(0)
        elif distance == 2:
            relay(1, 1, onward=False)
            relay(1, 2, across_too=False)
    if tall > 1:
        relay(2, 1, across_too=False)
    if tall > 2:
        relay(1, 2, onward=False)
    if tall > 1:
        slab_relay(1)
    ready(0)
    for distance in range(3, tall):
        relay(1, distance)
    project(0, 0)
    spread(2, z)
    if tall > 1:
        relay(2, 1, onward=False)
    if tall > 2:
        relay(2, 2)
        slab_relay(2)
    ready(1)
    for distance in range(3, tall):
        relay(2, distance)
    project(1, 0)
    for copy in tokens:
        copy.wait_recv()
    for number in range(2):
        for side in range(1, broad):
            project(number, side)
    for distance in range(3, tall):
        slab_relay(distance)
    slabs_of_z_along_y()
    slab_spread(y)
    ready(2)
    for side in range(broad):
        project(2, side)

    def split(values):
        first = values.astype(jnp.bfloat16).astype(jnp.float32)
        rest = values - first
        second = rest.astype(jnp.bfloat16).astype(jnp.float32)
        return first, second, rest - second

    block_lane = lax.broadcasted_iota(jnp.int32, (block, 2 * width), 1)
    ones_rows = jnp.where(lax.broadcasted_iota(jnp.int32, (16, block), 0) == 0, 1.0, 0.0)
    packed = wide == 2 * width

    def aside(head):
        return width if packed and head == 0 else 0

    def beside(head):
        low = aside(head)
        return (block_lane >= low) & (block_lane < low + width)

    def with_lanes(values, head, lanes):
        if packed:
            return jnp.where(beside(head), lanes, values.astype(jnp.float32)).astype(jnp.bfloat16)
        own = values[:, head * width : (head + 1) * width].astype(jnp.float32)
        return jnp.concatenate([lanes[:, :width], own], axis=1).astype(jnp.bfloat16)

    def query_operand(values, head):
        low = aside(head)
        ones = jnp.where((block_lane >= low) & (block_lane < low + 3), 1.0, 0.0)
        return with_lanes(values, head, ones)

    def key_operands(values, decay):
        sub = lax.broadcasted_iota(jnp.int32, (2 * width, block), 0)
        lanes = jnp.zeros((2 * width, block), jnp.float32)
        fresh = []
        for head in range(heads):
            for index, piece in enumerate(split(-decay[head : head + 1, :])):
                lanes = jnp.where(sub == aside(head) + index, piece, lanes)
            if not packed:
                fresh.append(with_lanes(values, head, lanes.T))
        if packed:
            turned = lanes.T
            fresh = [with_lanes(values, head, turned) for head in range(heads)]
        return fresh

    def value_operands(values):
        turned = values.astype(jnp.float32).T
        return [
            jnp.concatenate(
                [turned[head * width : (head + 1) * width], ones_rows], axis=0
            ).astype(jnp.bfloat16)
            for head in range(heads)
        ]

    def averages(parts):
        mixed, logs = [], []
        for peak, total in parts:
            norm = total[width : width + 1]
            mixed.append(total[:width] / norm)
            logs.append(peak + jnp.log(norm))
        return mixed, logs

    def pieces(values):
        return [
            (pltpu.roll(values, block - column * rows, 1) if column else values)[:, :rows]
            for column in range(broad)
        ]

    def stacked(rows_of, extent):
        sub = lax.broadcasted_iota(jnp.int32, (extent, block), 0)
        result = jnp.zeros((extent, block), jnp.float32)
        for index, piece in enumerate(rows_of):
            result = jnp.where(sub == index, piece, result)
        return result

    def scores_of(keys, queries):
        return lax.dot_general(keys, queries, DIMS_NT, preferred_element_type=jnp.float32)

    def online(carry, keys, queries, values):
        peak, total = carry
        scores = scores_of(keys, queries)
        higher = jnp.maximum(peak, jnp.max(scores, axis=0, keepdims=True))
        probs = jnp.exp(scores - higher).astype(jnp.bfloat16)
        total = total * jnp.exp(peak - higher) + jnp.dot(
            values, probs, preferred_element_type=jnp.float32
        )
        return higher, total

    def near_copy(turn, side):
        column = along_y(side)
        return remote(
            near_stage_ref.at[turn, column], near_ref.at[plane(turn) * broad + y],
            near_send.at[turn, side], near_recv.at[plane(turn) * broad + y],
            {"sp": z * broad + column},
        )

    key_place = lax.broadcasted_iota(jnp.int32, (block, block), 0)
    query_place = lax.broadcasted_iota(jnp.int32, (block, block), 1)

    def near_block(turn, unused):
        keys = key_operands(stage_ref[0, turn], home_decay_ref[plane(turn)])
        values = value_operands(stage_ref[1, turn])
        parts = []
        for head in range(heads):
            scores = scores_of(keys[head], query_operand(stage_ref[2, turn], head))
            scores = jnp.where(key_place <= query_place, scores, -jnp.inf)
            peak = jnp.max(scores, axis=0, keepdims=True)
            probs = jnp.exp(scores - peak).astype(jnp.bfloat16)
            parts.append(
                (peak, jnp.dot(values[head], probs, preferred_element_type=jnp.float32))
            )
        mixed, logs = averages(parts)
        tail = stacked([piece for log in logs for piece in split(log)], 16)
        for column, piece in enumerate(pieces(jnp.concatenate([*mixed, tail], axis=0))):
            near_stage_ref[turn, column] = piece.astype(jnp.bfloat16)
        near_ref[plane(turn) * broad + y] = near_stage_ref[turn, y]
        for side in range(1, broad):
            near_copy(turn, side).start()

        return unused

    for turn in range(1, tall):
        remote(
            home_decay_ref.at[plane(turn)], home_decay_ref.at[plane(turn)], decay_send.at[turn],
            decay_recv.at[plane(turn)], {"sp": me},
        ).wait_recv()
    slabs_from_y()
    lax.fori_loop(0, tall, near_block, 0)

    def prepare(level):
        moved(0, level)
        moved(1, level)
        place = pl.ds(pl.multiple_of(level * block, block), block)
        keys = key_operands(full_ref[0, place, :], decay_ref[:, place])
        values = value_operands(full_ref[1, place, :])
        for head in range(heads):
            key_ref[head, level] = keys[head]
            value_ref[head, level] = values[head]

    def remote_done(level, column):
        device = {"sp": level * broad + column}
        return [
            remote(
                done_ref.at[level, column], merged_ref.at[me], done_send.at[level, column],
                done_recv.at[me], device,
            ),
            remote(
                log_ref.at[level, column], logs_ref.at[me], log_send.at[level, column],
                log_recv.at[me], device,
            ),
        ]

    def far_block(index, unused):
        level = (index + 1) % max(tall - 1, 1) + 1
        for column in range(tall - 1):
            if index == max(column - 1, 0):
                prepare(column)

        moved(2, level)
        place = pl.ds(pl.multiple_of(level * block, block), block)
        queries = [query_operand(full_ref[2, place, :], head) for head in range(heads)]

        def step(column, carry):
            return tuple(
                online(carry[head], key_ref[head, column], queries[head], value_ref[head, column])
                for head in range(heads)
            )

        start = tuple(
            (
                jnp.full((1, block), -1e30, jnp.float32),
                jnp.zeros((width + 16, block), jnp.float32),
            )
            for _ in range(heads)
        )
        carry = start
        for column in range(level):
            carry = step(column, carry)
        mixed, logs = averages(carry)
        turned = jnp.concatenate(mixed, axis=0).T.astype(jnp.bfloat16)
        for column, piece in enumerate(pieces(stacked(logs, 8))):
            log_ref[level, column] = piece
            done_ref[level, column] = turned[column * rows : (column + 1) * rows]

            @pl.when(level * broad + column != me)
            def _():
                for copy in remote_done(level, column):
                    copy.start()

        if index == min(1, tall - 2):
            slabs_from_x()

        return unused

    for index in range(tall - 1):
        far_block(index, 0)

    @pl.when(z > 0)
    def _():
        merged_ref[me] = done_ref[z, y]
        logs_ref[me] = log_ref[z, y]
        for shift in range(1, count):
            source = lax.rem(me + shift, count)
            remote(
                merged_ref.at[source], merged_ref.at[source], done_send.at[0, 0],
                done_recv.at[source], {"sp": source},
            ).wait_recv()
            remote(
                logs_ref.at[source], logs_ref.at[source], log_send.at[0, 0],
                log_recv.at[source], {"sp": source},
            ).wait_recv()

    @pl.when(z == 0)
    def _():
        for source in range(count):
            merged_ref[source] = jnp.zeros((rows, wide), jnp.bfloat16)
            logs_ref[source] = jnp.full((8, rows), -1e30, jnp.float32)

    for turn in range(tall):
        for side in range(1, broad):
            target = near_ref.at[plane(turn) * broad + along_y(side)]
            remote(
                target, target, near_send.at[turn, side],
                near_recv.at[plane(turn) * broad + along_y(side)], {"sp": me},
            ).wait_recv()
    slabs_from_core()

    def combined(source):
        one = near_ref[source].astype(jnp.float32)
        two = merged_ref[source].astype(jnp.float32).T
        outs = []
        for head in range(heads):
            low = wide + 3 * head
            near_log = sum(one[low + i : low + i + 1] for i in range(3))
            logs = near_log, logs_ref[source][head : head + 1]
            peak = jnp.maximum(*logs)
            first, second = (jnp.exp(log - peak) for log in logs)
            norm = first + second
            place = slice(head * width, (head + 1) * width)
            mixed = one[place] * (first / norm) + two[place] * (second / norm)
            scale = lax.rsqrt(jnp.mean(mixed * mixed, axis=0, keepdims=True) + EPS)
            outs.append(mixed * scale)
        return jnp.concatenate(outs, axis=0).T.astype(jnp.bfloat16)

    merged = jnp.concatenate(
        [combined(level * broad + column) for column in range(broad) for level in range(tall)],
        axis=1,
    )
    columns = slab_ref.shape[1]
    for place in range(groups):
        out_ref[:, place * columns : (place + 1) * columns] = jnp.dot(
            merged, slabs_ref[place].reshape(-1, columns), preferred_element_type=jnp.float32
        ).astype(out_ref.dtype)

    for copy in tokens:
        copy.wait_send()
    for number in range(3):
        weights_sent(number)

        @pl.when(needed(number, z))
        def _():
            for side in range(broad):
                for turn in range(1, tall):
                    move(number, turn, side).wait_send()
    for turn in range(tall):
        if turn:
            home_decay(turn).wait_send()
        for side in range(1, broad):
            near_copy(turn, side).wait_send()
    for distance in range(tall):
        for way in range(2):
            level = z - distance if way == 0 else z + distance
            inside = (level >= 0) if way == 0 else (level < tall)
            onward = (z + 1 < tall) if way == 0 else (z > 0)

            @pl.when(inside & onward)
            def _():
                slab_z(level, way).wait_send()

    for shift in range(1, broad):
        slab_y(shift).wait_send()
    for column in range(broad):
        for shift in range(1, across):
            slab_x(column, shift).wait_send()
        for level in range(across):
            slab_core(level, column).wait_send()
    for level in range(1, tall):
        for column in range(broad):
            @pl.when(level * broad + column != me)
            def _():
                for copy in remote_done(level, column):
                    copy.wait_send()


def on_device(tokens, w_query, w_key, w_value, w_output, qk_gain, decay_sums):
    own_rows, decay_rows = tokens[0], decay_sums[0]
    count, groups = lax.axis_size("sp"), lax.axis_size("dp")
    tall, broad, across = layout(count, groups)
    rows, depth = own_rows.shape
    part = w_query.shape[0]
    heads, width = decay_rows.shape[0], qk_gain.shape[1]
    wide, length, block = heads * width, count * rows, broad * rows
    tall_slab, columns = w_output.shape
    bf16, sem, span = jnp.bfloat16, pltpu.SemaphoreType.DMA, wide + 16
    others, beside = max(broad - 1, 1), max(across - 1, 1)
    result = pl.pallas_call(
        functools.partial(layer_kernel, heads, width, count, groups),
        out_shape=jax.ShapeDtypeStruct((rows, depth), bf16),
        in_specs=[pl.BlockSpec(memory_space=pltpu.VMEM)] * 7,
        out_specs=pl.BlockSpec(memory_space=pltpu.VMEM),
        scratch_shapes=[
            pltpu.VMEM((others, rows, depth), bf16),
            pltpu.VMEM((3, tall, groups, part, wide), bf16),
            pltpu.VMEM((groups, broad, tall * tall_slab, columns), bf16),
            pltpu.VMEM((3, tall, block, wide), bf16),
            pltpu.VMEM((3, length, wide), bf16),
            pltpu.VMEM((heads, tall, block, 2 * width), bf16),
            pltpu.VMEM((heads, tall, width + 16, block), bf16),
            pltpu.VMEM((tall, heads, block), jnp.float32),
            pltpu.VMEM((tall, broad, span, rows), bf16),
            pltpu.VMEM((count, span, rows), bf16),
            pltpu.VMEM((tall, broad, rows, wide), bf16),
            pltpu.VMEM((count, rows, wide), bf16),
            pltpu.VMEM((tall, broad, 8, rows), jnp.float32),
            pltpu.VMEM((count, 8, rows), jnp.float32),
            sem((others,)), sem((others,)),
            sem((3, tall, 2)), sem((3, tall, beside)), sem((3, tall, across)),
            sem((3, tall, groups)),
            sem((3, broad, tall)), sem((3, count)),
            sem((tall, 2)), sem((tall,)), sem((others,)), sem((broad,)),
            sem((broad, beside)), sem((across, broad)), sem((across, broad)), sem((across, broad)),
            sem((tall, broad)), sem((count,)),
            sem((tall, broad)), sem((count,)), sem((tall,)), sem((tall,)),
            sem((tall, broad)), sem((count,)),
        ],
        compiler_params=pltpu.CompilerParams(
            collective_id=0, has_side_effects=True, vmem_limit_bytes=60 * 1024 * 1024
        ),
    )(own_rows, w_query, w_key, w_value, w_output, qk_gain, decay_rows)
    return result[None]


def solution(mesh):
    placed = (
        P("dp", "sp", None),
        P("dp", "sp"),
        P("dp", "sp"),
        P("dp", "sp"),
        P("sp", "dp"),
        P(),
        P("dp", "sp", None),
    )
    return jax.shard_map(
        on_device, mesh=mesh, in_specs=placed, out_specs=P("dp", "sp", None), check_vma=False
    )
```
